32 devices in a mesh: sp: 8 (over z, x), tp: 4 (over y, core).
Axes of the slice: x: 2, y: 2, z: 4, core: 2. Of those that a mesh axis runs over, the one named last changes fastest.
Arguments:
- stream: bfloat16 [4096, 2048], P(('sp', 'tp')), may hold values from -6 to 6
- queries: bfloat16 [4096, 512], P('sp', 'tp'), may hold values from -6 to 6
- key_rows: bfloat16 [4096, 512], P('sp', 'tp'), may hold values from -6 to 6
- values: bfloat16 [4096, 1024], P('sp', 'tp'), may hold values from -6 to 6
- out_gate: bfloat16 [4096, 1024], P('sp', 'tp'), may hold values from -6 to 6
- fwd_decay: float32 [4096, 512], P('sp', 'tp'), may hold values from -14 to 14
- bwd_decay: float32 [4096, 512], P('sp', 'tp'), may hold values from -14 to 14
- head_gain: float32 [1024], P('tp'), may hold values from 0.1 to 1.9
- out_proj: bfloat16 [1024, 2048], replicated, may hold values from -0.1875 to 0.1875
- mix_gain: float32 [2048], replicated, may hold values from 0.1 to 1.9
- ffn_gain: float32 [2048], replicated, may hold values from 0.1 to 1.9
- moe_gain: float32 [2048], replicated, may hold values from 0.1 to 1.9
- routes: int32 [4096, 2], P(('sp', 'tp')), may hold values from 0 to 7, all different within a row; in each aligned block of 128 rows (0 to 127, 128 to 255, ...) at most 48 rows name the same one
- route_weight: float32 [4096, 2], P(('sp', 'tp')), may hold values from 0.25 to 2.5
- expert_gate: bfloat16 [8, 2048, 1024], P('sp', None, 'tp'), may hold values from -0.125 to 0.125
- expert_up: bfloat16 [8, 2048, 1024], P('sp', None, 'tp'), may hold values from -0.125 to 0.125
- expert_down: bfloat16 [8, 1024, 2048], P('sp', 'tp'), may hold values from -0.1875 to 0.1875
- shared_gate: bfloat16 [2048, 512], P(None, 'tp'), may hold values from -0.125 to 0.125
- shared_up: bfloat16 [2048, 512], P(None, 'tp'), may hold values from -0.125 to 0.125
- shared_down: bfloat16 [512, 2048], P('tp'), may hold values from -0.25 to 0.25
Outputs:
- updated: bfloat16 [4096, 2048], P(('sp', 'tp'))
The draws below stay inside these ranges and needn't reach their ends.
Inputs may be any that keep to these rules, and one draw needn't show every extreme that they name: `routes`: each row names 2 different experts. Among the rows of one device no expert is named more than 48 times, and in every draw some device names some expert exactly 48 times.
All inputs are finite; a program needn't handle non-finite values.
Results may differ from the reference program's by a relative error of at most 0.023.
Values may be sent and summed in bfloat16 or wider, within the bound.
A program may use at most 128 MiB of HBM per device.

```python
import math
import jax
import jax.numpy as jnp
import numpy as np
from jax import lax

D = 2048
HEAD_TOTAL = 8
KEY_CHANNELS = 64
DV = 128
BLK = 64
FE = 1024
SH = 512
TOPK = 2
TOK_DEV = 128
TOKEN_COUNT = 4096
HV = 1024
EXPERTS = 8
CAP = 48
PARTS_SIZE = 4


def decay_law(key):
    head_key, chan_key, dev_key, jitter_key, position_key, fraction_key = jax.random.split(key, 6)
    slow_share = 0.5
    slow_heads = jax.random.uniform(head_key, (HEAD_TOTAL,)) < slow_share
    head_rate = jnp.where(slow_heads, 0.6 / TOKEN_COUNT, 2.5 / BLK)
    channel_rate = jnp.repeat(head_rate, KEY_CHANNELS) * jnp.exp(jax.random.uniform(chan_key, (HEAD_TOTAL * KEY_CHANNELS,), minval=-0.5, maxval=0.5))
    device_factor = jnp.exp(jax.random.uniform(dev_key, (TOKEN_COUNT // TOK_DEV, 1), minval=-0.7, maxval=0.7))
    rates = jnp.repeat(device_factor, TOK_DEV, axis=0) * channel_rate[None, :]
    preactivation = -jnp.log(jnp.expm1(16.0 * rates))
    preactivation = preactivation + jax.random.uniform(jitter_key, (TOKEN_COUNT, HEAD_TOTAL * KEY_CHANNELS), minval=-1.0, maxval=1.0)
    spike_rows = jax.random.randint(position_key, (2,), 0, TOKEN_COUNT)
    spike_fraction = jax.random.uniform(fraction_key, (2, HEAD_TOTAL * KEY_CHANNELS), minval=0.2, maxval=0.5)
    spike_preactivation = -jnp.log(jnp.expm1(-16.0 * jnp.log(1.0 - spike_fraction)))
    preactivation = preactivation.at[spike_rows].set(spike_preactivation)
    return jnp.clip(preactivation, -14.0, 14.0).astype(jnp.float32)


def draw_fwd_decay(key, part):
    return decay_law(jax.random.fold_in(key, 11))


def draw_bwd_decay(key, part):
    return decay_law(jax.random.fold_in(key, 23))


def levels(own_key, dims, cuts, low, high):
    gain = 1.0
    for dim, blocks in cuts:
        draws = jax.random.uniform(jax.random.fold_in(jax.random.fold_in(own_key, 6), dim), (blocks,), jnp.float32, low / len(cuts), high / len(cuts))
        gain = gain * jnp.repeat(jnp.exp(draws), dims[dim] // blocks).reshape((-1,) + (1,) * (len(dims) - 1 - dim))
    return gain


def deal_out(key, own, number, rows, amount, top, most, lean):
    sequence = jax.random.permutation(key, amount)
    heavy_load, ordinary = portions_of(amount, rows * top, most, lean, True), portions_of(amount, rows * top, most, lean, False)
    places = jnp.arange(amount)

    def named(tallies, rotation):
        used = int((tallies > 0).sum())
        fixed = max(1, used // 4)
        shifted = fixed + (places - fixed + rotation * (used - fixed)) % max(1, amount - fixed)
        return jnp.zeros((amount,), jnp.int32).at[sequence[jnp.where(places < fixed, places, shifted)]].set(jnp.asarray(tallies, jnp.int32))

    tallies = jnp.where(number % 4 == 0, named(heavy_load, number // 4), named(ordinary, number - number // 4 - 1))
    mixed = jax.random.permutation(jax.random.fold_in(own, 3), amount)
    giver, taker = mixed[0:amount // 2 * 2:2], mixed[1:amount // 2 * 2:2]
    room = jnp.minimum(tallies[giver] - 1, most - tallies[taker]) // 2
    room = jnp.where((giver == sequence[0]) | (taker == sequence[0]) | (tallies[taker] == 0), 0, jnp.maximum(room, 0))
    shifted = jax.random.randint(jax.random.fold_in(own, 4), (amount // 2,), 0, 1 << 20) % (room + 1)
    tallies = tallies.at[giver].add(-shifted).at[taker].add(shifted)
    members = jnp.searchsorted(jnp.cumsum(tallies), jnp.arange(rows * top), side="right").astype(jnp.int32)
    listing = members.reshape(top, rows).T
    listing = listing[jax.random.permutation(jax.random.fold_in(own, 1), rows)]
    rotation = jax.random.randint(jax.random.fold_in(own, 2), (rows, 1), 0, top)
    return jnp.take_along_axis(listing, (jnp.arange(top)[None, :] + rotation) % top, axis=1)


def portions_of(count, total, reach, skew, full):
    weights = [(1 << 20) // math.isqrt(standing ** skew) + 1 for standing in range(1, count + 1)]
    largest = reach if full else min(reach, max(-(-total // count), total * weights[0] // sum(weights)))
    least = 1 if total - largest >= count - 1 else 0
    given, surplus = [largest] + [least] * (count - 1), total - largest - least * (count - 1)
    while surplus > 0:
        free = [i for i in range(1, count) if given[i] < largest] or [i for i in range(1, count) if given[i] < reach]
        mass, left = sum([weights[i] for i in free]), surplus
        for i in free:
            extra = min(reach - given[i], max(1, left * weights[i] // mass), surplus)
            given[i] = given[i] + extra
            surplus = surplus - extra
    return np.array(given)


def bell_draw(own_key, dims, width, most, cuts=(), kind=jnp.bfloat16):
    drawn = jax.random.normal(own_key, dims, jnp.float32) * width
    if len(cuts) > 0:
        drawn = levels(own_key, dims, cuts, -0.22, 0.18) * drawn
    return jnp.clip(drawn, min=-most, max=most).astype(kind)


def setup_inputs(seed: int = 0) -> dict:
    arg_keys = jax.random.split(jax.random.key(seed), 21)
    stream = bell_draw(arg_keys[0], (TOKEN_COUNT, D), 1.0, 6.0, ((0, 32),))
    queries = bell_draw(arg_keys[1], (TOKEN_COUNT, HEAD_TOTAL * KEY_CHANNELS), 1.0, 6.0, ((0, 8), (1, 4)))
    key_rows = bell_draw(arg_keys[2], (TOKEN_COUNT, HEAD_TOTAL * KEY_CHANNELS), 1.0, 6.0, ((0, 8), (1, 4)))
    values = bell_draw(arg_keys[3], (TOKEN_COUNT, HV), 1.0, 6.0, ((0, 8), (1, 4)))
    out_gate = bell_draw(arg_keys[4], (TOKEN_COUNT, HV), 1.0, 6.0, ((0, 8), (1, 4)))
    fwd_decay = draw_fwd_decay(jax.random.fold_in(arg_keys[20], 71), 0)
    bwd_decay = draw_bwd_decay(jax.random.fold_in(arg_keys[20], 71), 0)
    head_gain = jnp.clip(1.0 + 0.18 * jax.random.normal(arg_keys[7], (HV,), jnp.float32), 0.1, 1.9)
    out_proj = bell_draw(arg_keys[8], (HV, D), HV ** -0.5, 0.1875)
    mix_gain = jnp.clip(1.0 + 0.18 * jax.random.normal(arg_keys[9], (D,), jnp.float32), 0.1, 1.9)
    ffn_gain = jnp.clip(1.0 + 0.18 * jax.random.normal(arg_keys[10], (D,), jnp.float32), 0.1, 1.9)
    moe_gain = jnp.clip(1.0 + 0.18 * jax.random.normal(arg_keys[11], (D,), jnp.float32), 0.1, 1.9)
    routes_keys = jax.random.split(jax.random.fold_in(arg_keys[12], 1), TOKEN_COUNT // TOK_DEV)
    routes_turns = jax.random.permutation(jax.random.fold_in(arg_keys[12], 3), TOKEN_COUNT // TOK_DEV)
    routes = jax.vmap(lambda own, number: deal_out(jax.random.fold_in(arg_keys[12], 2), own, number, TOK_DEV, EXPERTS, TOPK, CAP, 1))(routes_keys, routes_turns).reshape((TOKEN_COUNT, TOPK))
    route_weight = jnp.clip(jnp.exp(math.log(2.5) - 2.3025851 * jax.random.uniform(arg_keys[13], (TOKEN_COUNT, TOPK), jnp.float32) ** levels(arg_keys[13], (TOKEN_COUNT, TOPK), ((0, 32),), -0.2, 0.2)), 0.25, 2.5)
    expert_gate = bell_draw(arg_keys[14], (EXPERTS, D, FE), D ** -0.5, 0.125, ((0, 8), (2, 4)))
    expert_up = bell_draw(arg_keys[15], (EXPERTS, D, FE), D ** -0.5, 0.125, ((0, 8), (2, 4)))
    expert_down = bell_draw(arg_keys[16], (EXPERTS, FE, D), FE ** -0.5, 0.1875, ((0, 8), (1, 4)))
    shared_gate = bell_draw(arg_keys[17], (D, SH), D ** -0.5, 0.125, ((1, 4),))
    shared_up = bell_draw(arg_keys[18], (D, SH), D ** -0.5, 0.125, ((1, 4),))
    shared_down = bell_draw(arg_keys[19], (SH, D), SH ** -0.5, 0.25, ((0, 4),))
    return {"stream": stream, "queries": queries, "key_rows": key_rows, "values": values, "out_gate": out_gate, "fwd_decay": fwd_decay, "bwd_decay": bwd_decay, "head_gain": head_gain, "out_proj": out_proj, "mix_gain": mix_gain, "ffn_gain": ffn_gain, "moe_gain": moe_gain, "routes": routes, "route_weight": route_weight, "expert_gate": expert_gate, "expert_up": expert_up, "expert_down": expert_down, "shared_gate": shared_gate, "shared_up": shared_up, "shared_down": shared_down}


EPS = 1e-06
GATE_NORM = 16.0
ROPE_BASE = 10000.0
TOP_PRECISION = lax.Precision.HIGHEST

def normalize(tensor):
    return tensor * lax.rsqrt(lax.optimization_barrier(jnp.mean(tensor * tensor, axis=-1, keepdims=True)) + EPS)

def rotate(tensor, positions):
    half_width = tensor.shape[-1] // 2
    frequency = ROPE_BASE ** (-jnp.arange(half_width, dtype=jnp.float32) / half_width)
    angles = positions[:, None] * frequency[None, :]
    cosine = jnp.cos(angles)[:, None, :]
    sine_part = jnp.sin(angles)[:, None, :]
    front_half = tensor[..., :half_width]
    back_half = tensor[..., half_width:]
    return jnp.concatenate([front_half * cosine - back_half * sine_part, front_half * sine_part + back_half * cosine], axis=-1)

def blockwise(query_rows, key_data, value_matrix, log_decay, start_state):
    length, head_count, key_width = query_rows.shape
    value_width = value_matrix.shape[-1]
    block_count = length // BLK
    query_blocks = query_rows.reshape(block_count, BLK, head_count, key_width)
    key_blocks = key_data.reshape(block_count, BLK, head_count, key_width)
    value_blocks = value_matrix.reshape(block_count, BLK, head_count, value_width)
    cumul = jnp.cumsum(log_decay.reshape(block_count, BLK, head_count, key_width), axis=1)
    middle = cumul[:, BLK // 2 - 1:BLK // 2]
    query_scaled = query_blocks * jnp.exp(cumul - middle)
    key_scaled = key_blocks * jnp.exp(middle - cumul)
    scores = jnp.einsum('nthk,nshk->nhts', query_scaled, key_scaled, precision=TOP_PRECISION)
    lower_mask = jnp.arange(BLK)[:, None] >= jnp.arange(BLK)[None, :]
    scores = jnp.where(lower_mask, scores, 0.0)
    within = jnp.einsum('nhts,nshv->nthv', scores, value_blocks, precision=TOP_PRECISION)
    last_cumul = cumul[:, -1:]
    query_in = query_blocks * jnp.exp(cumul)
    key_out = key_blocks * jnp.exp(last_cumul - cumul)
    block_decay = jnp.exp(last_cumul[:, 0])

    def advance(carried_state, pieces):
        query_segment, key_segment, value_segment, decay_segment = pieces
        across_blocks = jnp.einsum('asu,sun->asn', query_segment, carried_state, precision=TOP_PRECISION)
        carried_state = carried_state * decay_segment[:, :, None] + jnp.einsum('jco,jcm->com', key_segment, value_segment, precision=TOP_PRECISION)
        return (carried_state, across_blocks)
    final_state, across_blocks = lax.scan(advance, start_state, (query_in, key_out, value_blocks, block_decay))
    return ((within + across_blocks).reshape(length, head_count, value_width), final_state)

def reference(stream, queries, key_rows, values, out_gate, fwd_decay, bwd_decay, head_gain, out_proj, mix_gain, ffn_gain, moe_gain, routes, route_weight, expert_gate, expert_up, expert_down, shared_gate, shared_up, shared_down):
    positions = jnp.arange(TOKEN_COUNT, dtype=jnp.int32).astype(jnp.float32)
    query_rows = rotate(queries.astype(jnp.float32).reshape(TOKEN_COUNT, HEAD_TOTAL, KEY_CHANNELS) * KEY_CHANNELS ** (-0.5), positions)
    key_data = rotate(key_rows.astype(jnp.float32).reshape(TOKEN_COUNT, HEAD_TOTAL, KEY_CHANNELS), positions)
    value_matrix = values.astype(jnp.float32).reshape(TOKEN_COUNT, HEAD_TOTAL, DV)
    fwd_log = jax.nn.log_sigmoid(fwd_decay).reshape(TOKEN_COUNT, HEAD_TOTAL, KEY_CHANNELS) / GATE_NORM
    bwd_log = jax.nn.log_sigmoid(bwd_decay).reshape(TOKEN_COUNT, HEAD_TOTAL, KEY_CHANNELS) / GATE_NORM
    zero_state = jnp.zeros((HEAD_TOTAL, KEY_CHANNELS, DV), jnp.float32)
    fwd_out, _ = blockwise(query_rows, key_data, value_matrix, fwd_log, zero_state)
    bwd_out, _ = blockwise(query_rows[::-1], key_data[::-1], value_matrix[::-1], bwd_log[::-1], zero_state)
    combined = normalize(fwd_out + bwd_out[::-1]) * head_gain.reshape(HEAD_TOTAL, DV)
    mixed_out = (combined.reshape(TOKEN_COUNT, HV) * jax.nn.silu(out_gate.astype(jnp.float32))).astype(jnp.bfloat16)
    projected = jnp.dot(mixed_out, out_proj, preferred_element_type=jnp.float32)
    residual = (stream.astype(jnp.float32) + normalize(projected) * mix_gain).astype(jnp.bfloat16)
    normed = (normalize(residual.astype(jnp.float32)) * ffn_gain).astype(jnp.bfloat16)
    shared_hidden = (jax.nn.silu(jnp.dot(normed, shared_gate, preferred_element_type=jnp.float32)) * jnp.dot(normed, shared_up, preferred_element_type=jnp.float32)).astype(jnp.bfloat16)
    group_width = SH // PARTS_SIZE
    shared_out = jnp.zeros((TOKEN_COUNT, D), jnp.float32)
    for quarter in range(PARTS_SIZE):
        piece = jnp.dot(shared_hidden[:, quarter * group_width:(quarter + 1) * group_width], shared_down[quarter * group_width:(quarter + 1) * group_width], preferred_element_type=jnp.float32)
        shared_out = shared_out + lax.optimization_barrier(piece.astype(jnp.bfloat16)).astype(jnp.float32)
    row_block = 256
    flat_ids = routes.reshape(-1)
    grand_total = flat_ids.shape[0]
    token_index = jnp.arange(grand_total, dtype=jnp.int32) // TOPK
    sort_order = jnp.argsort(flat_ids, stable=True)
    sorted_expert = flat_ids[sort_order]
    sorted_token = token_index[sort_order]
    sorted_weight = route_weight.reshape(-1)[sort_order]
    counts = lax.optimization_barrier(jnp.sum((flat_ids[:, None] == jnp.arange(EXPERTS, dtype=jnp.int32)[None, :]).astype(jnp.int32), axis=0))
    starts = jnp.cumsum(counts) - counts
    padded = (counts + row_block - 1) // row_block * row_block
    block_ends = jnp.cumsum(padded)
    padded_starts = block_ends - padded
    position = (padded_starts[sorted_expert] + jnp.arange(grand_total, dtype=jnp.int32) - starts[sorted_expert]).astype(jnp.int32)
    block_total = -(-(grand_total + EXPERTS * (row_block - 1)) // row_block)
    slot_token = jnp.zeros((block_total * row_block,), jnp.int32).at[position].set(sorted_token)
    slot_weight = jnp.zeros((block_total * row_block,), jnp.float32).at[position].set(sorted_weight)
    block_expert = jnp.minimum(jnp.searchsorted(block_ends, jnp.arange(block_total, dtype=jnp.int32) * row_block, side='right'), EXPERTS - 1).astype(jnp.int32)
    expert_width = FE // PARTS_SIZE

    def add_block(totals, block_item):
        token_ids, slot_wts, expert = block_item
        row_data = normed[token_ids]
        gate_mat = lax.dynamic_index_in_dim(expert_gate, expert, 0, keepdims=False)
        up_mat = lax.dynamic_index_in_dim(expert_up, expert, 0, keepdims=False)
        down_mat = lax.dynamic_index_in_dim(expert_down, expert, 0, keepdims=False)
        hidden = (jax.nn.silu(jnp.dot(row_data, gate_mat, preferred_element_type=jnp.float32)) * jnp.dot(row_data, up_mat, preferred_element_type=jnp.float32)).astype(jnp.bfloat16)
        quarter_sums = jnp.einsum('rqf,qfd->qrd', hidden.astype(jnp.float32).reshape(row_block, PARTS_SIZE, expert_width), down_mat.astype(jnp.float32).reshape(PARTS_SIZE, expert_width, D), precision=TOP_PRECISION)
        rounded = lax.optimization_barrier(quarter_sums.astype(jnp.bfloat16)).astype(jnp.float32)
        result = lax.optimization_barrier(lax.optimization_barrier(jnp.sum(rounded, axis=0)).astype(jnp.bfloat16)).astype(jnp.float32)
        return (totals.at[token_ids].add(result * slot_wts[:, None]), None)
    routed_sum, _ = lax.scan(add_block, jnp.zeros((TOKEN_COUNT, D), jnp.float32), (slot_token.reshape(block_total, row_block), slot_weight.reshape(block_total, row_block), block_expert))
    mixture = shared_out + routed_sum
    return (residual.astype(jnp.float32) + normalize(mixture) * moe_gain).astype(jnp.bfloat16)
```

```python
import jax
import jax.numpy as jnp
from jax import lax
from jax.sharding import PartitionSpec as P

KEY_CHANNELS = 64
DV = 128
BLK = 64
TOPK = 2


EPS = 1e-06
GATE_NORM = 16.0
ROPE_BASE = 10000.0
TOP_PRECISION = lax.Precision.HIGHEST


def carried_in(fwd_summary, bwd_summary, axis):
    count = lax.axis_size(axis)
    place = lax.axis_index(axis)
    decays = jnp.stack([fwd_summary[0], bwd_summary[0]])
    states = jnp.stack([fwd_summary[1], bwd_summary[1]])
    width = states.shape[-1]
    packed = jnp.concatenate(
        [states.reshape(-1, width), decays.reshape(-1, width)], axis=0
    ).astype(jnp.bfloat16)
    gathered = lax.all_gather(packed, axis).astype(jnp.float32)
    state_rows = states.size // width
    all_states = gathered[:, :state_rows].reshape((count,) + states.shape)
    all_decays = gathered[:, state_rows:].reshape((count,) + decays.shape)
    fwd = jnp.zeros_like(states[0])
    bwd = jnp.zeros_like(states[0])
    for step in range(count):
        fwd = jnp.where(
            step < place, fwd * all_decays[step, 0][:, :, None] + all_states[step, 0], fwd
        )
        source = count - 1 - step
        bwd = jnp.where(
            source > place, bwd * all_decays[source, 1][:, :, None] + all_states[source, 1], bwd
        )
    return fwd, bwd


def normalize(tensor):
    return tensor * lax.rsqrt(jnp.mean(tensor * tensor, axis=-1, keepdims=True) + EPS)


def rotate(tensor, positions):
    half_width = tensor.shape[-1] // 2
    frequency = ROPE_BASE ** (-jnp.arange(half_width, dtype=jnp.float32) / half_width)
    angles = positions[:, None] * frequency[None, :]
    cosine = jnp.cos(angles)[:, None, :]
    sine_part = jnp.sin(angles)[:, None, :]
    front_half = tensor[..., :half_width]
    back_half = tensor[..., half_width:]
    return jnp.concatenate(
        [front_half * cosine - back_half * sine_part, front_half * sine_part + back_half * cosine],
        axis=-1,
    )


def blockwise(query_rows, key_data, value_matrix, log_decay, start_state):
    length, head_count, key_width = query_rows.shape
    value_width = value_matrix.shape[-1]
    block_count = length // BLK
    query_blocks = query_rows.reshape(block_count, BLK, head_count, key_width)
    key_blocks = key_data.reshape(block_count, BLK, head_count, key_width)
    value_blocks = value_matrix.reshape(block_count, BLK, head_count, value_width)
    cumul = jnp.cumsum(log_decay.reshape(block_count, BLK, head_count, key_width), axis=1)
    middle = cumul[:, BLK // 2 - 1 : BLK // 2]
    query_scaled = query_blocks * jnp.exp(cumul - middle)
    key_scaled = key_blocks * jnp.exp(middle - cumul)
    scores = jnp.einsum("nthk,nshk->nhts", query_scaled, key_scaled, precision=TOP_PRECISION)
    lower_mask = jnp.arange(BLK)[:, None] >= jnp.arange(BLK)[None, :]
    scores = jnp.where(lower_mask, scores, 0.0)
    within = jnp.einsum("nhts,nshv->nthv", scores, value_blocks, precision=TOP_PRECISION)
    last_cumul = cumul[:, -1:]
    query_in = query_blocks * jnp.exp(cumul)
    key_out = key_blocks * jnp.exp(last_cumul - cumul)
    block_decay = jnp.exp(last_cumul[:, 0])

    def advance(carried_state, pieces):
        query_segment, key_segment, value_segment, decay_segment = pieces
        across_blocks = jnp.einsum(
            "asu,sun->asn", query_segment, carried_state, precision=TOP_PRECISION
        )
        carried_state = carried_state * decay_segment[:, :, None] + jnp.einsum(
            "jco,jcm->com", key_segment, value_segment, precision=TOP_PRECISION
        )
        return (carried_state, across_blocks)

    final_state, across_blocks = lax.scan(
        advance,
        start_state,
        (query_in, key_out, value_blocks, block_decay),
        unroll=block_count,
    )
    return ((within + across_blocks).reshape(length, head_count, value_width), final_state)


def summarize(key_data, value_matrix, log_decay):
    cumul = jnp.cumsum(log_decay, axis=0)
    grand_total = cumul[-1]
    weighted_rows = key_data * jnp.exp(grand_total[None] - cumul)
    return (
        jnp.exp(grand_total),
        jnp.einsum("jco,jcm->com", weighted_rows, value_matrix, precision=TOP_PRECISION),
    )


def feed_forward(row_data, gate_parts, up_parts, down_mat):
    groups, _, width = gate_parts.shape
    total = jnp.zeros((row_data.shape[0], down_mat.shape[1]), jnp.float32)
    for group in range(groups):
        hidden = (
            jax.nn.silu(jnp.dot(row_data, gate_parts[group], preferred_element_type=jnp.float32))
            * jnp.dot(row_data, up_parts[group], preferred_element_type=jnp.float32)
        ).astype(jnp.bfloat16)
        total = total + jnp.dot(
            hidden,
            down_mat[group * width : (group + 1) * width],
            preferred_element_type=jnp.float32,
        )
    return total


def slot_map(route_block, experts, capacity):
    tokens, choices = route_block.shape
    flat_ids = route_block.reshape(-1)
    total = flat_ids.shape[0]
    onehot = (flat_ids[:, None] == jnp.arange(experts, dtype=jnp.int32)[None, :]).astype(
        jnp.bfloat16
    )
    earlier = (jnp.arange(total)[:, None] > jnp.arange(total)[None, :]).astype(jnp.bfloat16)
    before = jnp.dot(earlier, onehot, preferred_element_type=jnp.float32)
    slot_ids = jnp.sum(before * onehot.astype(jnp.float32), axis=1).astype(jnp.int32)
    return (flat_ids * capacity + slot_ids).reshape(tokens, choices)


def body(
    stream,
    queries,
    key_rows,
    values,
    out_gate,
    fwd_decay,
    bwd_decay,
    head_gain,
    out_proj,
    mix_gain,
    ffn_gain,
    moe_gain,
    routes,
    route_weight,
    expert_gate,
    expert_up,
    expert_down,
    shared_gate,
    shared_up,
    shared_down,
):
    tokens_here = stream.shape[0]
    span_rows = queries.shape[0]
    heads_here = queries.shape[1] // KEY_CHANNELS
    experts = lax.axis_size("sp")
    capacity = max(2, 3 * tokens_here * TOPK // (2 * experts))
    gate_parts = lax.all_gather(expert_gate[0], "tp")
    up_parts = lax.all_gather(expert_up[0], "tp")
    down_mat = lax.all_gather(expert_down[0], "tp", axis=0, tiled=True)
    shared_gate_parts = lax.all_gather(shared_gate, "tp")
    shared_up_parts = lax.all_gather(shared_up, "tp")
    shared_down_mat = lax.all_gather(shared_down, "tp", axis=0, tiled=True)
    rows_of = slot_map(routes, experts, capacity)
    slots = jnp.arange(experts * capacity, dtype=jnp.int32)
    taken = rows_of[:, :, None] == slots[None, None, :]
    pick = jnp.any(taken, axis=1).astype(jnp.bfloat16)
    weights = jnp.sum(jnp.where(taken, route_weight[:, :, None], 0.0), axis=1)
    weights_high = weights.astype(jnp.bfloat16)
    weights_low = (weights - weights_high.astype(jnp.float32)).astype(jnp.bfloat16)
    offset = lax.axis_index("sp") * span_rows
    positions = (offset + jnp.arange(span_rows, dtype=jnp.int32)).astype(jnp.float32)
    query_rows = rotate(
        queries.astype(jnp.float32).reshape(span_rows, heads_here, KEY_CHANNELS)
        * KEY_CHANNELS ** (-0.5),
        positions,
    )
    key_data = rotate(
        key_rows.astype(jnp.float32).reshape(span_rows, heads_here, KEY_CHANNELS), positions
    )
    value_matrix = values.astype(jnp.float32).reshape(span_rows, heads_here, DV)
    fwd_log = jax.nn.log_sigmoid(fwd_decay).reshape(span_rows, heads_here, KEY_CHANNELS) / GATE_NORM
    bwd_log = (
        jax.nn.log_sigmoid(bwd_decay[::-1]).reshape(span_rows, heads_here, KEY_CHANNELS) / GATE_NORM
    )
    query_back = query_rows[::-1]
    key_back = key_data[::-1]
    value_back = value_matrix[::-1]
    fwd_summary = summarize(key_data, value_matrix, fwd_log)
    bwd_summary = summarize(key_back, value_back, bwd_log)
    fwd_carry, bwd_carry = carried_in(fwd_summary, bwd_summary, "sp")
    fwd_out, _ = blockwise(query_rows, key_data, value_matrix, fwd_log, fwd_carry)
    bwd_out, _ = blockwise(query_back, key_back, value_back, bwd_log, bwd_carry)
    combined = normalize(fwd_out + bwd_out[::-1]) * head_gain.reshape(heads_here, DV)
    head_mixed = (
        combined.reshape(span_rows, -1) * jax.nn.silu(out_gate.astype(jnp.float32))
    ).astype(jnp.bfloat16)
    mixed_out = lax.all_to_all(head_mixed, "tp", split_axis=0, concat_axis=1, tiled=True)
    projected = jnp.dot(mixed_out, out_proj, preferred_element_type=jnp.float32)
    residual = (stream.astype(jnp.float32) + normalize(projected) * mix_gain).astype(jnp.bfloat16)
    normed = (normalize(residual.astype(jnp.float32)) * ffn_gain).astype(jnp.bfloat16)
    model_width = normed.shape[1]
    outgoing = lax.dot_general(
        pick, normed, (((0,), (0,)), ((), ())), preferred_element_type=jnp.float32
    ).astype(jnp.bfloat16)
    arrived = lax.all_to_all(
        outgoing.reshape(experts, capacity, model_width),
        "sp",
        split_axis=0,
        concat_axis=0,
        tiled=True,
    )
    shared_sum = feed_forward(normed, shared_gate_parts, shared_up_parts, shared_down_mat)
    routed_done = feed_forward(
        arrived.reshape(experts * capacity, model_width), gate_parts, up_parts, down_mat
    ).astype(jnp.bfloat16)
    routed_back = lax.all_to_all(
        routed_done.reshape(experts, capacity, model_width),
        "sp",
        split_axis=0,
        concat_axis=0,
        tiled=True,
    ).reshape(experts * capacity, model_width)
    mixture = (
        shared_sum
        + jnp.dot(weights_high, routed_back, preferred_element_type=jnp.float32)
        + jnp.dot(weights_low, routed_back, preferred_element_type=jnp.float32)
    )
    return (residual.astype(jnp.float32) + normalize(mixture) * moe_gain).astype(jnp.bfloat16)


def solution(mesh):
    return jax.shard_map(
        body,
        mesh=mesh,
        in_specs=(
            P(("sp", "tp"), None),
            P("sp", "tp"),
            P("sp", "tp"),
            P("sp", "tp"),
            P("sp", "tp"),
            P("sp", "tp"),
            P("sp", "tp"),
            P("tp"),
            P(),
            P(),
            P(),
            P(),
            P(("sp", "tp"), None),
            P(("sp", "tp"), None),
            P("sp", None, "tp"),
            P("sp", None, "tp"),
            P("sp", "tp", None),
            P(None, "tp"),
            P(None, "tp"),
            P("tp", None),
        ),
        out_specs=P(("sp", "tp"), None),
        check_vma=False,
    )
```

```python
import functools

import jax
import jax.numpy as jnp
from jax import lax
from jax.experimental import pallas as pl
from jax.experimental.pallas import tpu as pltpu
from jax.sharding import PartitionSpec as P

KEY_CHANNELS = 64
DV = 128
BLK = 64
TOPK = 2


EPS = 1e-06
GATE_NORM = 16.0
ROPE_BASE = 10000.0
TOP_PRECISION = lax.Precision.HIGHEST
MESH = pl.DeviceIdType.MESH


def normalize(tensor):
    return tensor * lax.rsqrt(jnp.mean(tensor * tensor, axis=-1, keepdims=True) + EPS)


def dot_nt(left, right):
    return lax.dot_general(
        left, right, (((1,), (1,)), ((), ())), preferred_element_type=jnp.float32
    )


def dot_tn(left, right):
    return lax.dot_general(
        left, right, (((0,), (0,)), ((), ())), preferred_element_type=jnp.float32
    )


def attention_kernel(
    sp_count,
    tp_count,
    q_ref,
    k_ref,
    v_ref,
    gate_ref,
    fwd_ref,
    bwd_ref,
    cos_ref,
    sin_ref,
    gain_ref,
    out_ref,
    own_ref,
    got_ref,
    mixed_ref,
    land_ref,
    within_ref,
    key_ref,
    sums_f,
    sums_b,
    sum_send,
    sum_recv,
    row_send,
    row_recv,
):
    span, lanes = q_ref.shape
    width = v_ref.shape[1]
    heads = lanes // KEY_CHANNELS
    blocks = span // BLK
    rows_out = span // tp_count
    sp_me = lax.axis_index("sp")
    tp_me = lax.axis_index("tp")

    barrier = pltpu.get_barrier_semaphore()
    for step in range(1, sp_count):
        pl.semaphore_signal(
            barrier,
            inc=1,
            device_id=(lax.rem(sp_me + step, sp_count), tp_me),
            device_id_type=MESH,
        )
    for step in range(1, tp_count):
        pl.semaphore_signal(
            barrier,
            inc=1,
            device_id=(sp_me, lax.rem(tp_me + step, tp_count)),
            device_id_type=MESH,
        )

    row = lax.broadcasted_iota(jnp.int32, (BLK, BLK), 0)
    column = lax.broadcasted_iota(jnp.int32, (BLK, BLK), 1)
    lower = row >= column
    upper = row <= column
    lower_ones = lower.astype(jnp.float32)
    upper_ones = upper.astype(jnp.float32)
    from_lane = lax.broadcasted_iota(jnp.int32, (lanes, lanes), 0)
    to_lane = lax.broadcasted_iota(jnp.int32, (lanes, lanes), 1)
    half = KEY_CHANNELS // 2
    partner = jnp.where(lax.rem(to_lane, KEY_CHANNELS) < half, to_lane + half, to_lane - half)
    swap = (from_lane == partner).astype(jnp.bfloat16)
    own_head = (
        lax.broadcasted_iota(jnp.int32, (width, lanes), 0) // DV
        == lax.broadcasted_iota(jnp.int32, (width, lanes), 1) // KEY_CHANNELS
    )
    lane_head = lax.broadcasted_iota(jnp.int32, (BLK, lanes), 1) // KEY_CHANNELS

    def rotated(tensor, rows):
        swapped = jnp.dot(tensor, swap, preferred_element_type=jnp.float32)
        return tensor.astype(jnp.float32) * cos_ref[rows, :] + swapped * sin_ref[rows, :]

    cumul_f, cumul_b, decay_f, decay_b = [], [], [], []
    for block in range(blocks):
        rows = pl.ds(block * BLK, BLK)
        total_f = jnp.dot(
            lower_ones, fwd_ref[rows, :], precision=TOP_PRECISION, preferred_element_type=jnp.float32
        )
        total_b = jnp.dot(
            upper_ones, bwd_ref[rows, :], precision=TOP_PRECISION, preferred_element_type=jnp.float32
        )
        last_f = total_f[BLK - 1 : BLK]
        last_b = total_b[0:1]
        keys = rotated(k_ref[rows, :], rows)
        key_ref[rows, :] = keys
        value_rows = v_ref[rows, :]
        out_f = (keys * jnp.exp(last_f - total_f)).astype(jnp.bfloat16)
        out_b = (keys * jnp.exp(last_b - total_b)).astype(jnp.bfloat16)
        sums_f[block] = jnp.where(own_head, dot_tn(value_rows, out_f), 0.0)
        sums_b[block] = jnp.where(own_head, dot_tn(value_rows, out_b), 0.0)
        cumul_f.append(total_f)
        cumul_b.append(total_b)
        decay_f.append(jnp.exp(last_f))
        decay_b.append(jnp.exp(last_b))

    def packed(total):
        return sum(total[h * DV : (h + 1) * DV] for h in range(heads))

    total = sums_f[0]
    through = decay_f[0]
    for block in range(1, blocks):
        total = total * decay_f[block] + sums_f[block]
        through = through * decay_f[block]
    own_ref[0:DV, :] = packed(total).astype(jnp.bfloat16)
    own_ref[2 * DV : 2 * DV + 8, :] = jnp.broadcast_to(through, (8, lanes)).astype(jnp.bfloat16)
    total = sums_b[blocks - 1]
    through = decay_b[blocks - 1]
    for block in range(blocks - 2, -1, -1):
        total = total * decay_b[block] + sums_b[block]
        through = through * decay_b[block]
    own_ref[DV : 2 * DV, :] = packed(total).astype(jnp.bfloat16)
    own_ref[2 * DV + 8 : 2 * DV + 16, :] = jnp.broadcast_to(through, (8, lanes)).astype(
        jnp.bfloat16
    )

    pl.semaphore_wait(barrier, sp_count - 1 + tp_count - 1)
    sum_copies = []
    for step in range(1, sp_count):
        copy = pltpu.make_async_remote_copy(
            src_ref=own_ref,
            dst_ref=got_ref.at[step],
            send_sem=sum_send.at[step],
            recv_sem=sum_recv.at[step],
            device_id=(lax.rem(sp_me + step, sp_count), tp_me),
            device_id_type=MESH,
        )
        copy.start()
        sum_copies.append(copy)

    query_f, query_b = [], []
    for block in range(blocks):
        rows = pl.ds(block * BLK, BLK)
        queries = rotated(q_ref[rows, :], rows) * KEY_CHANNELS ** (-0.5)
        keys = key_ref[rows, :]
        total_f, total_b = cumul_f[block], cumul_b[block]
        middle_f = total_f[BLK // 2 - 1 : BLK // 2]
        middle_b = total_b[BLK // 2 : BLK // 2 + 1]
        scaled_qf = queries * jnp.exp(total_f - middle_f)
        scaled_qb = queries * jnp.exp(total_b - middle_b)
        scaled_kf = (keys * jnp.exp(middle_f - total_f)).astype(jnp.bfloat16)
        scaled_kb = (keys * jnp.exp(middle_b - total_b)).astype(jnp.bfloat16)
        query_f.append((queries * jnp.exp(total_f)).astype(jnp.bfloat16))
        query_b.append((queries * jnp.exp(total_b)).astype(jnp.bfloat16))
        for h in range(heads):
            mine = lane_head == h
            scores_f = dot_nt(jnp.where(mine, scaled_qf, 0.0).astype(jnp.bfloat16), scaled_kf)
            scores_b = dot_nt(jnp.where(mine, scaled_qb, 0.0).astype(jnp.bfloat16), scaled_kb)
            scores = jnp.where(lower, scores_f, 0.0) + jnp.where(upper, scores_b, 0.0)
            within_ref[rows, h * DV : (h + 1) * DV] = jnp.dot(
                scores.astype(jnp.bfloat16),
                v_ref[rows, h * DV : (h + 1) * DV],
                preferred_element_type=jnp.float32,
            )

    for copy in sum_copies:
        copy.wait()
    carry_f = jnp.zeros((DV, lanes), jnp.float32)
    carry_b = jnp.zeros((DV, lanes), jnp.float32)
    for step in range(sp_count - 1, 0, -1):
        state = got_ref[step, 0:DV, :].astype(jnp.float32)
        through = got_ref[step, 2 * DV : 2 * DV + 16, :].astype(jnp.float32)[0:1]
        carry_f = jnp.where(step <= sp_me, carry_f * through + state, carry_f)
    for step in range(1, sp_count):
        state = got_ref[step, DV : 2 * DV, :].astype(jnp.float32)
        through = got_ref[step, 2 * DV : 2 * DV + 16, :].astype(jnp.float32)[8:9]
        carry_b = jnp.where(step > sp_me, carry_b * through + state, carry_b)

    def unpacked(carry):
        return jnp.where(own_head, jnp.concatenate([carry] * heads, axis=0), 0.0)

    state = unpacked(carry_f)
    for block in range(blocks):
        rows = pl.ds(block * BLK, BLK)
        within_ref[rows, :] += dot_nt(query_f[block], state.astype(jnp.bfloat16))
        if block < blocks - 1:
            state = state * decay_f[block] + sums_f[block]
    state = unpacked(carry_b)
    for block in range(blocks - 1, -1, -1):
        rows = pl.ds(block * BLK, BLK)
        attended = within_ref[rows, :] + dot_nt(query_b[block], state.astype(jnp.bfloat16))
        if block > 0:
            state = state * decay_b[block] + sums_b[block]
        for h in range(heads):
            part = attended[:, h * DV : (h + 1) * DV]
            square = jnp.mean(part * part, axis=-1, keepdims=True)
            gate = gate_ref[rows, h * DV : (h + 1) * DV].astype(jnp.float32)
            mixed_ref[rows, h * DV : (h + 1) * DV] = (
                part
                * lax.rsqrt(square + EPS)
                * gain_ref[:, h * DV : (h + 1) * DV]
                * (gate / (1.0 + jnp.exp(-gate)))
            ).astype(jnp.bfloat16)

    row_copies = []
    for step in range(1, tp_count):
        target = lax.rem(tp_me + step, tp_count)
        copy = pltpu.make_async_remote_copy(
            src_ref=mixed_ref.at[pl.ds(pl.multiple_of(target * rows_out, rows_out), rows_out)],
            dst_ref=land_ref.at[tp_me],
            send_sem=row_send.at[step],
            recv_sem=row_recv.at[step],
            device_id=(sp_me, target),
            device_id_type=MESH,
        )
        copy.start()
        row_copies.append(copy)
    land_ref[tp_me] = mixed_ref[pl.ds(pl.multiple_of(tp_me * rows_out, rows_out), rows_out), :]
    for copy in row_copies:
        copy.wait()
    for source in range(tp_count):
        out_ref[:, source * width : (source + 1) * width] = land_ref[source]


def attention(queries, key_rows, values, out_gate, fwd_log, bwd_log, cosine, signed_sine, gain):
    sp_count = lax.axis_size("sp")
    tp_count = lax.axis_size("tp")
    span, lanes = queries.shape
    width = values.shape[1]
    rows_out = span // tp_count
    blocks = span // BLK
    vmem = pl.BlockSpec(memory_space=pltpu.VMEM)
    return pl.pallas_call(
        functools.partial(attention_kernel, sp_count, tp_count),
        out_shape=jax.ShapeDtypeStruct((rows_out, tp_count * width), jnp.bfloat16),
        in_specs=[vmem] * 9,
        out_specs=vmem,
        scratch_shapes=[
            pltpu.VMEM((2 * DV + 16, lanes), jnp.bfloat16),
            pltpu.VMEM((sp_count, 2 * DV + 16, lanes), jnp.bfloat16),
            pltpu.VMEM((span, width), jnp.bfloat16),
            pltpu.VMEM((tp_count, rows_out, width), jnp.bfloat16),
            pltpu.VMEM((span, width), jnp.float32),
            pltpu.VMEM((span, lanes), jnp.float32),
            pltpu.VMEM((blocks, width, lanes), jnp.float32),
            pltpu.VMEM((blocks, width, lanes), jnp.float32),
            pltpu.SemaphoreType.DMA((sp_count,)),
            pltpu.SemaphoreType.DMA((sp_count,)),
            pltpu.SemaphoreType.DMA((tp_count,)),
            pltpu.SemaphoreType.DMA((tp_count,)),
        ],
        compiler_params=pltpu.CompilerParams(collective_id=0, has_side_effects=True),
    )(queries, key_rows, values, out_gate, fwd_log, bwd_log, cosine, signed_sine, gain)


def feed_forward(row_data, gate_parts, up_parts, down_mat):
    groups, _, width = gate_parts.shape
    total = jnp.zeros((row_data.shape[0], down_mat.shape[1]), jnp.float32)
    for group in range(groups):
        hidden = (
            jax.nn.silu(jnp.dot(row_data, gate_parts[group], preferred_element_type=jnp.float32))
            * jnp.dot(row_data, up_parts[group], preferred_element_type=jnp.float32)
        ).astype(jnp.bfloat16)
        total = total + jnp.dot(
            hidden,
            down_mat[group * width : (group + 1) * width],
            preferred_element_type=jnp.float32,
        )
    return total


def slot_map(route_block, experts, capacity):
    tokens, choices = route_block.shape
    flat_ids = route_block.reshape(-1)
    total = flat_ids.shape[0]
    onehot = (flat_ids[:, None] == jnp.arange(experts, dtype=jnp.int32)[None, :]).astype(
        jnp.bfloat16
    )
    earlier = (jnp.arange(total)[:, None] > jnp.arange(total)[None, :]).astype(jnp.bfloat16)
    before = jnp.dot(earlier, onehot, preferred_element_type=jnp.float32)
    slot_ids = jnp.sum(before * onehot.astype(jnp.float32), axis=1).astype(jnp.int32)
    return (flat_ids * capacity + slot_ids).reshape(tokens, choices)


def body(
    stream,
    queries,
    key_rows,
    values,
    out_gate,
    fwd_decay,
    bwd_decay,
    head_gain,
    out_proj,
    mix_gain,
    ffn_gain,
    moe_gain,
    routes,
    route_weight,
    expert_gate,
    expert_up,
    expert_down,
    shared_gate,
    shared_up,
    shared_down,
):
    tokens_here = stream.shape[0]
    span_rows = queries.shape[0]
    experts = lax.axis_size("sp")
    capacity = max(2, 3 * tokens_here * TOPK // (2 * experts))
    gate_parts = lax.all_gather(expert_gate[0], "tp")
    up_parts = lax.all_gather(expert_up[0], "tp")
    down_mat = lax.all_gather(expert_down[0], "tp", axis=0, tiled=True)
    shared_width = shared_gate.shape[1]
    shared_all = lax.all_gather(
        jnp.concatenate([shared_gate, shared_up, shared_down.T], axis=1), "tp"
    )
    rows_of = slot_map(routes, experts, capacity)
    slots = jnp.arange(experts * capacity, dtype=jnp.int32)
    taken = rows_of[:, :, None] == slots[None, None, :]
    pick = jnp.any(taken, axis=1).astype(jnp.bfloat16)
    weights = jnp.sum(jnp.where(taken, route_weight[:, :, None], 0.0), axis=1)
    weights_high = weights.astype(jnp.bfloat16)
    weights_low = (weights - weights_high.astype(jnp.float32)).astype(jnp.bfloat16)
    offset = lax.axis_index("sp") * span_rows
    positions = (offset + jnp.arange(span_rows, dtype=jnp.int32)).astype(jnp.float32)
    lanes = queries.shape[1]
    half = KEY_CHANNELS // 2
    lane = jnp.arange(lanes, dtype=jnp.int32) % KEY_CHANNELS
    frequency = ROPE_BASE ** (-(lane % half).astype(jnp.float32) / half)
    angles = positions[:, None] * frequency[None, :]
    sine = jnp.sin(angles)
    mixed_out = attention(
        queries,
        key_rows,
        values,
        out_gate,
        jax.nn.log_sigmoid(fwd_decay) / GATE_NORM,
        jax.nn.log_sigmoid(bwd_decay) / GATE_NORM,
        jnp.cos(angles),
        jnp.where(lane[None, :] < half, -sine, sine),
        head_gain.reshape(1, -1),
    )
    projected = jnp.dot(mixed_out, out_proj, preferred_element_type=jnp.float32)
    residual = (stream.astype(jnp.float32) + normalize(projected) * mix_gain).astype(jnp.bfloat16)
    normed = (normalize(residual.astype(jnp.float32)) * ffn_gain).astype(jnp.bfloat16)
    model_width = normed.shape[1]
    outgoing = lax.dot_general(
        pick, normed, (((0,), (0,)), ((), ())), preferred_element_type=jnp.float32
    ).astype(jnp.bfloat16)
    arrived = lax.all_to_all(
        outgoing.reshape(experts, capacity, model_width),
        "sp",
        split_axis=0,
        concat_axis=0,
        tiled=True,
    )
    shared_sum = jnp.zeros((tokens_here, model_width), jnp.float32)
    for group in range(lax.axis_size("tp")):
        both = jnp.dot(
            normed, shared_all[group, :, : 2 * shared_width], preferred_element_type=jnp.float32
        )
        hidden = (jax.nn.silu(both[:, :shared_width]) * both[:, shared_width:]).astype(
            jnp.bfloat16
        )
        shared_sum = shared_sum + dot_nt(hidden, shared_all[group, :, 2 * shared_width :])
    routed_done = feed_forward(
        arrived.reshape(experts * capacity, model_width), gate_parts, up_parts, down_mat
    ).astype(jnp.bfloat16)
    routed_back = lax.all_to_all(
        routed_done.reshape(experts, capacity, model_width),
        "sp",
        split_axis=0,
        concat_axis=0,
        tiled=True,
    ).reshape(experts * capacity, model_width)
    mixture = (
        shared_sum
        + jnp.dot(weights_high, routed_back, preferred_element_type=jnp.float32)
        + jnp.dot(weights_low, routed_back, preferred_element_type=jnp.float32)
    )
    return (residual.astype(jnp.float32) + normalize(mixture) * moe_gain).astype(jnp.bfloat16)


def solution(mesh):
    return jax.shard_map(
        body,
        mesh=mesh,
        in_specs=(
            P(("sp", "tp"), None),
            P("sp", "tp"),
            P("sp", "tp"),
            P("sp", "tp"),
            P("sp", "tp"),
            P("sp", "tp"),
            P("sp", "tp"),
            P("tp"),
            P(),
            P(),
            P(),
            P(),
            P(("sp", "tp"), None),
            P(("sp", "tp"), None),
            P("sp", None, "tp"),
            P("sp", None, "tp"),
            P("sp", "tp", None),
            P(None, "tp"),
            P(None, "tp"),
            P("tp", None),
        ),
        out_specs=P(("sp", "tp"), None),
        check_vma=False,
    )
```

```python
import functools

import jax
import jax.numpy as jnp
from jax import lax
from jax.experimental import pallas as pl
from jax.experimental.pallas import tpu as pltpu
from jax.sharding import PartitionSpec as P

KEY_CHANNELS = 64
DV = 128
BLK = 64
TOPK = 2


EPS = 1e-06
GATE_NORM = 16.0
ROPE_BASE = 10000.0
TOP_PRECISION = lax.Precision.HIGHEST
MESH = pl.DeviceIdType.MESH


def normalize(tensor):
    return tensor * lax.rsqrt(jnp.mean(tensor * tensor, axis=-1, keepdims=True) + EPS)


def dot_nt(left, right):
    return lax.dot_general(
        left, right, (((1,), (1,)), ((), ())), preferred_element_type=jnp.float32
    )


def dot_tn(left, right):
    return lax.dot_general(
        left, right, (((0,), (0,)), ((), ())), preferred_element_type=jnp.float32
    )


def attention_kernel(
    sp_count,
    tp_count,
    q_ref,
    k_ref,
    v_ref,
    gate_ref,
    fwd_ref,
    bwd_ref,
    cos_ref,
    sin_ref,
    gain_ref,
    out_ref,
    own_ref,
    got_ref,
    mixed_ref,
    land_ref,
    within_ref,
    key_ref,
    sums_f,
    sums_b,
    sum_send,
    sum_recv,
    row_send,
    row_recv,
):
    span, lanes = q_ref.shape
    width = v_ref.shape[1]
    heads = lanes // KEY_CHANNELS
    blocks = span // BLK
    rows_out = span // tp_count
    sp_me = lax.axis_index("sp")
    tp_me = lax.axis_index("tp")

    barrier = pltpu.get_barrier_semaphore()
    for step in range(1, sp_count):
        pl.semaphore_signal(
            barrier,
            inc=1,
            device_id=(lax.rem(sp_me + step, sp_count), tp_me),
            device_id_type=MESH,
        )
    for step in range(1, tp_count):
        pl.semaphore_signal(
            barrier,
            inc=1,
            device_id=(sp_me, lax.rem(tp_me + step, tp_count)),
            device_id_type=MESH,
        )

    row = lax.broadcasted_iota(jnp.int32, (BLK, BLK), 0)
    column = lax.broadcasted_iota(jnp.int32, (BLK, BLK), 1)
    lower = row >= column
    upper = row <= column
    lower_ones = lower.astype(jnp.float32)
    upper_ones = upper.astype(jnp.float32)
    from_lane = lax.broadcasted_iota(jnp.int32, (lanes, lanes), 0)
    to_lane = lax.broadcasted_iota(jnp.int32, (lanes, lanes), 1)
    half = KEY_CHANNELS // 2
    partner = jnp.where(lax.rem(to_lane, KEY_CHANNELS) < half, to_lane + half, to_lane - half)
    swap = (from_lane == partner).astype(jnp.bfloat16)
    own_head = (
        lax.broadcasted_iota(jnp.int32, (width, lanes), 0) // DV
        == lax.broadcasted_iota(jnp.int32, (width, lanes), 1) // KEY_CHANNELS
    )
    lane_head = lax.broadcasted_iota(jnp.int32, (BLK, lanes), 1) // KEY_CHANNELS

    def rotated(tensor, rows):
        swapped = jnp.dot(tensor, swap, preferred_element_type=jnp.float32)
        return tensor.astype(jnp.float32) * cos_ref[rows, :] + swapped * sin_ref[rows, :]

    cumul_f, cumul_b, decay_f, decay_b = [], [], [], []
    for block in range(blocks):
        rows = pl.ds(block * BLK, BLK)
        total_f = jnp.dot(
            lower_ones, fwd_ref[rows, :], precision=TOP_PRECISION, preferred_element_type=jnp.float32
        )
        total_b = jnp.dot(
            upper_ones, bwd_ref[rows, :], precision=TOP_PRECISION, preferred_element_type=jnp.float32
        )
        last_f = total_f[BLK - 1 : BLK]
        last_b = total_b[0:1]
        keys = rotated(k_ref[rows, :], rows)
        key_ref[rows, :] = keys
        value_rows = v_ref[rows, :]
        out_f = (keys * jnp.exp(last_f - total_f)).astype(jnp.bfloat16)
        out_b = (keys * jnp.exp(last_b - total_b)).astype(jnp.bfloat16)
        sums_f[block] = jnp.where(own_head, dot_tn(value_rows, out_f), 0.0)
        sums_b[block] = jnp.where(own_head, dot_tn(value_rows, out_b), 0.0)
        cumul_f.append(total_f)
        cumul_b.append(total_b)
        decay_f.append(jnp.exp(last_f))
        decay_b.append(jnp.exp(last_b))

    def packed(total):
        return sum(total[h * DV : (h + 1) * DV] for h in range(heads))

    total = sums_f[0]
    through = decay_f[0]
    for block in range(1, blocks):
        total = total * decay_f[block] + sums_f[block]
        through = through * decay_f[block]
    own_ref[0:DV, :] = packed(total).astype(jnp.bfloat16)
    own_ref[2 * DV : 2 * DV + 8, :] = jnp.broadcast_to(through, (8, lanes)).astype(jnp.bfloat16)
    total = sums_b[blocks - 1]
    through = decay_b[blocks - 1]
    for block in range(blocks - 2, -1, -1):
        total = total * decay_b[block] + sums_b[block]
        through = through * decay_b[block]
    own_ref[DV : 2 * DV, :] = packed(total).astype(jnp.bfloat16)
    own_ref[2 * DV + 8 : 2 * DV + 16, :] = jnp.broadcast_to(through, (8, lanes)).astype(
        jnp.bfloat16
    )

    pl.semaphore_wait(barrier, sp_count - 1 + tp_count - 1)
    sum_copies = []
    for step in range(1, sp_count):
        copy = pltpu.make_async_remote_copy(
            src_ref=own_ref,
            dst_ref=got_ref.at[step],
            send_sem=sum_send.at[step],
            recv_sem=sum_recv.at[step],
            device_id=(lax.rem(sp_me + step, sp_count), tp_me),
            device_id_type=MESH,
        )
        copy.start()
        sum_copies.append(copy)

    query_f, query_b = [], []
    for block in range(blocks):
        rows = pl.ds(block * BLK, BLK)
        queries = rotated(q_ref[rows, :], rows) * KEY_CHANNELS ** (-0.5)
        keys = key_ref[rows, :]
        total_f, total_b = cumul_f[block], cumul_b[block]
        middle_f = total_f[BLK // 2 - 1 : BLK // 2]
        middle_b = total_b[BLK // 2 : BLK // 2 + 1]
        scaled_qf = queries * jnp.exp(total_f - middle_f)
        scaled_qb = queries * jnp.exp(total_b - middle_b)
        scaled_kf = (keys * jnp.exp(middle_f - total_f)).astype(jnp.bfloat16)
        scaled_kb = (keys * jnp.exp(middle_b - total_b)).astype(jnp.bfloat16)
        query_f.append((queries * jnp.exp(total_f)).astype(jnp.bfloat16))
        query_b.append((queries * jnp.exp(total_b)).astype(jnp.bfloat16))
        for h in range(heads):
            mine = lane_head == h
            scores_f = dot_nt(jnp.where(mine, scaled_qf, 0.0).astype(jnp.bfloat16), scaled_kf)
            scores_b = dot_nt(jnp.where(mine, scaled_qb, 0.0).astype(jnp.bfloat16), scaled_kb)
            scores = jnp.where(lower, scores_f, 0.0) + jnp.where(upper, scores_b, 0.0)
            within_ref[rows, h * DV : (h + 1) * DV] = jnp.dot(
                scores.astype(jnp.bfloat16),
                v_ref[rows, h * DV : (h + 1) * DV],
                preferred_element_type=jnp.float32,
            )

    for copy in sum_copies:
        copy.wait()
    carry_f = jnp.zeros((DV, lanes), jnp.float32)
    carry_b = jnp.zeros((DV, lanes), jnp.float32)
    for step in range(sp_count - 1, 0, -1):
        state = got_ref[step, 0:DV, :].astype(jnp.float32)
        through = got_ref[step, 2 * DV : 2 * DV + 16, :].astype(jnp.float32)[0:1]
        carry_f = jnp.where(step <= sp_me, carry_f * through + state, carry_f)
    for step in range(1, sp_count):
        state = got_ref[step, DV : 2 * DV, :].astype(jnp.float32)
        through = got_ref[step, 2 * DV : 2 * DV + 16, :].astype(jnp.float32)[8:9]
        carry_b = jnp.where(step > sp_me, carry_b * through + state, carry_b)

    def unpacked(carry):
        return jnp.where(own_head, jnp.concatenate([carry] * heads, axis=0), 0.0)

    state = unpacked(carry_f)
    for block in range(blocks):
        rows = pl.ds(block * BLK, BLK)
        within_ref[rows, :] += dot_nt(query_f[block], state.astype(jnp.bfloat16))
        if block < blocks - 1:
            state = state * decay_f[block] + sums_f[block]
    state = unpacked(carry_b)
    for block in range(blocks - 1, -1, -1):
        rows = pl.ds(block * BLK, BLK)
        attended = within_ref[rows, :] + dot_nt(query_b[block], state.astype(jnp.bfloat16))
        if block > 0:
            state = state * decay_b[block] + sums_b[block]
        for h in range(heads):
            part = attended[:, h * DV : (h + 1) * DV]
            square = jnp.mean(part * part, axis=-1, keepdims=True)
            gate = gate_ref[rows, h * DV : (h + 1) * DV].astype(jnp.float32)
            mixed_ref[rows, h * DV : (h + 1) * DV] = (
                part
                * lax.rsqrt(square + EPS)
                * gain_ref[:, h * DV : (h + 1) * DV]
                * (gate / (1.0 + jnp.exp(-gate)))
            ).astype(jnp.bfloat16)

    row_copies = []
    for step in range(1, tp_count):
        target = lax.rem(tp_me + step, tp_count)
        copy = pltpu.make_async_remote_copy(
            src_ref=mixed_ref.at[pl.ds(pl.multiple_of(target * rows_out, rows_out), rows_out)],
            dst_ref=land_ref.at[tp_me],
            send_sem=row_send.at[step],
            recv_sem=row_recv.at[step],
            device_id=(sp_me, target),
            device_id_type=MESH,
        )
        copy.start()
        row_copies.append(copy)
    land_ref[tp_me] = mixed_ref[pl.ds(pl.multiple_of(tp_me * rows_out, rows_out), rows_out), :]
    for copy in row_copies:
        copy.wait()
    for source in range(tp_count):
        out_ref[:, source * width : (source + 1) * width] = land_ref[source]


def attention(queries, key_rows, values, out_gate, fwd_log, bwd_log, cosine, signed_sine, gain):
    sp_count = lax.axis_size("sp")
    tp_count = lax.axis_size("tp")
    span, lanes = queries.shape
    width = values.shape[1]
    rows_out = span // tp_count
    blocks = span // BLK
    vmem = pl.BlockSpec(memory_space=pltpu.VMEM)
    return pl.pallas_call(
        functools.partial(attention_kernel, sp_count, tp_count),
        out_shape=jax.ShapeDtypeStruct((rows_out, tp_count * width), jnp.bfloat16),
        in_specs=[vmem] * 9,
        out_specs=vmem,
        scratch_shapes=[
            pltpu.VMEM((2 * DV + 16, lanes), jnp.bfloat16),
            pltpu.VMEM((sp_count, 2 * DV + 16, lanes), jnp.bfloat16),
            pltpu.VMEM((span, width), jnp.bfloat16),
            pltpu.VMEM((tp_count, rows_out, width), jnp.bfloat16),
            pltpu.VMEM((span, width), jnp.float32),
            pltpu.VMEM((span, lanes), jnp.float32),
            pltpu.VMEM((blocks, width, lanes), jnp.float32),
            pltpu.VMEM((blocks, width, lanes), jnp.float32),
            pltpu.SemaphoreType.DMA((sp_count,)),
            pltpu.SemaphoreType.DMA((sp_count,)),
            pltpu.SemaphoreType.DMA((tp_count,)),
            pltpu.SemaphoreType.DMA((tp_count,)),
        ],
        compiler_params=pltpu.CompilerParams(collective_id=0, has_side_effects=True),
    )(queries, key_rows, values, out_gate, fwd_log, bwd_log, cosine, signed_sine, gain)


def dispatch_kernel(
    sp_count,
    tp_count,
    outgoing_ref,
    rows_ref,
    gate_ref,
    up_ref,
    down_ref,
    arrived_ref,
    shared_ref,
    block_land,
    row_land,
    part_ref,
    part_land,
    block_send,
    block_recv,
    row_send,
    row_recv,
    part_send,
    part_recv,
):
    sp_me = lax.axis_index("sp")
    tp_me = lax.axis_index("tp")

    def sp_peer(step):
        return (lax.rem(sp_me + step, sp_count), tp_me)

    def tp_peer(step):
        return (sp_me, lax.rem(tp_me + step, tp_count))

    barrier = pltpu.get_barrier_semaphore()
    for step in range(1, sp_count):
        pl.semaphore_signal(barrier, inc=1, device_id=sp_peer(step), device_id_type=MESH)
    for step in range(1, tp_count):
        pl.semaphore_signal(barrier, inc=1, device_id=tp_peer(step), device_id_type=MESH)
    pl.semaphore_wait(barrier, sp_count - 1 + tp_count - 1)

    row_copies, block_copies, part_copies = [], [], []
    for step in range(1, tp_count):
        copy = pltpu.make_async_remote_copy(
            src_ref=rows_ref,
            dst_ref=row_land.at[step],
            send_sem=row_send.at[step],
            recv_sem=row_recv.at[step],
            device_id=tp_peer(step),
            device_id_type=MESH,
        )
        copy.start()
        row_copies.append(copy)
    for step in range(1, sp_count):
        copy = pltpu.make_async_remote_copy(
            src_ref=outgoing_ref.at[lax.rem(sp_me + step, sp_count)],
            dst_ref=block_land.at[sp_me],
            send_sem=block_send.at[step],
            recv_sem=block_recv.at[step],
            device_id=sp_peer(step),
            device_id_type=MESH,
        )
        copy.start()
        block_copies.append(copy)
    block_land[sp_me] = outgoing_ref[sp_me]

    def partial(rows):
        hidden = jax.nn.silu(
            jnp.dot(rows, gate_ref[...], preferred_element_type=jnp.float32)
        ) * jnp.dot(rows, up_ref[...], preferred_element_type=jnp.float32)
        return jnp.dot(
            hidden.astype(jnp.bfloat16), down_ref[...], preferred_element_type=jnp.float32
        )

    shared_ref[...] = partial(rows_ref[...])
    for step in range(1, tp_count):
        row_copies[step - 1].wait()
        part_ref[step] = partial(row_land[step]).astype(jnp.bfloat16)
        copy = pltpu.make_async_remote_copy(
            src_ref=part_ref.at[step],
            dst_ref=part_land.at[step],
            send_sem=part_send.at[step],
            recv_sem=part_recv.at[step],
            device_id=tp_peer(tp_count - step),
            device_id_type=MESH,
        )
        copy.start()
        part_copies.append(copy)
    for step in range(1, tp_count):
        part_copies[step - 1].wait()
        shared_ref[...] += part_land[step].astype(jnp.float32)
    for copy in block_copies:
        copy.wait()
    arrived_ref[...] = block_land[...]


def dispatch(outgoing, normed, shared_gate, shared_up, shared_down):
    sp_count = lax.axis_size("sp")
    tp_count = lax.axis_size("tp")
    vmem = pl.BlockSpec(memory_space=pltpu.VMEM)
    several = pltpu.VMEM((tp_count,) + normed.shape, normed.dtype)
    return pl.pallas_call(
        functools.partial(dispatch_kernel, sp_count, tp_count),
        out_shape=(
            jax.ShapeDtypeStruct(outgoing.shape, outgoing.dtype),
            jax.ShapeDtypeStruct(normed.shape, jnp.float32),
        ),
        in_specs=[vmem] * 5,
        out_specs=(vmem, vmem),
        scratch_shapes=[
            pltpu.VMEM(outgoing.shape, outgoing.dtype),
            several,
            several,
            several,
            pltpu.SemaphoreType.DMA((sp_count,)),
            pltpu.SemaphoreType.DMA((sp_count,)),
            pltpu.SemaphoreType.DMA((tp_count,)),
            pltpu.SemaphoreType.DMA((tp_count,)),
            pltpu.SemaphoreType.DMA((tp_count,)),
            pltpu.SemaphoreType.DMA((tp_count,)),
        ],
        compiler_params=pltpu.CompilerParams(collective_id=1, has_side_effects=True),
    )(outgoing, normed, shared_gate, shared_up, shared_down)


def expert_kernel(
    sp_count,
    rows_ref,
    gate_hbm,
    up_hbm,
    down_hbm,
    high_ref,
    low_ref,
    shared_ref,
    residual_ref,
    gain_ref,
    out_ref,
    gate_ref,
    up_ref,
    down_ref,
    total_ref,
    done_ref,
    back_ref,
    weight_sem,
    send_sem,
    recv_sem,
):
    sp_me = lax.axis_index("sp")
    tp_me = lax.axis_index("tp")
    groups, _, width = gate_ref.shape
    capacity = done_ref.shape[1]

    fetches = []
    for group in range(groups):
        cut = pl.ds(group * width, width)
        trio = (
            pltpu.make_async_copy(gate_hbm.at[group], gate_ref.at[group], weight_sem.at[0, group]),
            pltpu.make_async_copy(up_hbm.at[group], up_ref.at[group], weight_sem.at[1, group]),
            pltpu.make_async_copy(down_hbm.at[cut], down_ref.at[cut], weight_sem.at[2, group]),
        )
        for copy in trio:
            copy.start()
        fetches.append(trio)

    barrier = pltpu.get_barrier_semaphore()
    for step in range(1, sp_count):
        pl.semaphore_signal(
            barrier,
            inc=1,
            device_id=(lax.rem(sp_me + step, sp_count), tp_me),
            device_id_type=MESH,
        )

    for group in range(groups):
        for copy in fetches[group]:
            copy.wait()
        hidden = (
            jax.nn.silu(jnp.dot(rows_ref[...], gate_ref[group], preferred_element_type=jnp.float32))
            * jnp.dot(rows_ref[...], up_ref[group], preferred_element_type=jnp.float32)
        ).astype(jnp.bfloat16)
        piece = jnp.dot(
            hidden,
            down_ref[group * width : (group + 1) * width, :],
            preferred_element_type=jnp.float32,
        )
        if group == 0:
            total_ref[...] = piece
        else:
            total_ref[...] += piece
    for source in range(sp_count):
        done_ref[source] = total_ref[source * capacity : (source + 1) * capacity, :].astype(
            done_ref.dtype
        )

    pl.semaphore_wait(barrier, sp_count - 1)
    copies = []
    for step in range(1, sp_count):
        target = lax.rem(sp_me + step, sp_count)
        copy = pltpu.make_async_remote_copy(
            src_ref=done_ref.at[target],
            dst_ref=back_ref.at[sp_me],
            send_sem=send_sem.at[step],
            recv_sem=recv_sem.at[step],
            device_id=(target, tp_me),
            device_id_type=MESH,
        )
        copy.start()
        copies.append(copy)
    back_ref[sp_me] = done_ref[sp_me]
    for copy in copies:
        copy.wait()

    mixture = shared_ref[...]
    for expert in range(sp_count):
        mixture = mixture + jnp.dot(
            high_ref[expert], back_ref[expert], preferred_element_type=jnp.float32
        )
        mixture = mixture + jnp.dot(
            low_ref[expert], back_ref[expert], preferred_element_type=jnp.float32
        )
    square = jnp.mean(mixture * mixture, axis=-1, keepdims=True)
    out_ref[...] = (
        residual_ref[...].astype(jnp.float32)
        + mixture * lax.rsqrt(square + EPS) * gain_ref[...]
    ).astype(out_ref.dtype)


def run_expert(rows, gate_parts, up_parts, down_mat, high, low, shared_sum, residual, gain):
    sp_count = lax.axis_size("sp")
    groups = gate_parts.shape[0]
    vmem = pl.BlockSpec(memory_space=pltpu.VMEM)
    hbm = pl.BlockSpec(memory_space=pl.ANY)
    blocked = pltpu.VMEM((sp_count, rows.shape[0] // sp_count, rows.shape[1]), rows.dtype)
    return pl.pallas_call(
        functools.partial(expert_kernel, sp_count),
        out_shape=jax.ShapeDtypeStruct(residual.shape, residual.dtype),
        in_specs=[vmem, hbm, hbm, hbm] + [vmem] * 5,
        out_specs=vmem,
        scratch_shapes=[
            pltpu.VMEM(gate_parts.shape, gate_parts.dtype),
            pltpu.VMEM(up_parts.shape, up_parts.dtype),
            pltpu.VMEM(down_mat.shape, down_mat.dtype),
            pltpu.VMEM(rows.shape, jnp.float32),
            blocked,
            blocked,
            pltpu.SemaphoreType.DMA((3, groups)),
            pltpu.SemaphoreType.DMA((sp_count,)),
            pltpu.SemaphoreType.DMA((sp_count,)),
        ],
        compiler_params=pltpu.CompilerParams(collective_id=2, has_side_effects=True),
    )(rows, gate_parts, up_parts, down_mat, high, low, shared_sum, residual, gain)


def slot_map(route_block, experts, capacity):
    tokens, choices = route_block.shape
    flat_ids = route_block.reshape(-1)
    total = flat_ids.shape[0]
    onehot = (flat_ids[:, None] == jnp.arange(experts, dtype=jnp.int32)[None, :]).astype(
        jnp.bfloat16
    )
    earlier = (jnp.arange(total)[:, None] > jnp.arange(total)[None, :]).astype(jnp.bfloat16)
    before = jnp.dot(earlier, onehot, preferred_element_type=jnp.float32)
    slot_ids = jnp.sum(before * onehot.astype(jnp.float32), axis=1).astype(jnp.int32)
    return (flat_ids * capacity + slot_ids).reshape(tokens, choices)


def body(
    stream,
    queries,
    key_rows,
    values,
    out_gate,
    fwd_decay,
    bwd_decay,
    head_gain,
    out_proj,
    mix_gain,
    ffn_gain,
    moe_gain,
    routes,
    route_weight,
    expert_gate,
    expert_up,
    expert_down,
    shared_gate,
    shared_up,
    shared_down,
):
    tokens_here = stream.shape[0]
    span_rows = queries.shape[0]
    experts = lax.axis_size("sp")
    capacity = max(2, 3 * tokens_here * TOPK // (2 * experts))
    gate_parts = lax.all_gather(expert_gate[0], "tp")
    up_parts = lax.all_gather(expert_up[0], "tp")
    down_mat = lax.all_gather(expert_down[0], "tp", axis=0, tiled=True)
    rows_of = slot_map(routes, experts, capacity)
    slots = jnp.arange(experts * capacity, dtype=jnp.int32)
    taken = rows_of[:, :, None] == slots[None, None, :]
    pick = jnp.any(taken, axis=1).astype(jnp.bfloat16)
    weights = jnp.sum(jnp.where(taken, route_weight[:, :, None], 0.0), axis=1)
    weights = weights.reshape(tokens_here, experts, capacity).transpose(1, 0, 2)
    weights_high = weights.astype(jnp.bfloat16)
    weights_low = (weights - weights_high.astype(jnp.float32)).astype(jnp.bfloat16)
    offset = lax.axis_index("sp") * span_rows
    positions = (offset + jnp.arange(span_rows, dtype=jnp.int32)).astype(jnp.float32)
    lanes = queries.shape[1]
    half = KEY_CHANNELS // 2
    lane = jnp.arange(lanes, dtype=jnp.int32) % KEY_CHANNELS
    frequency = ROPE_BASE ** (-(lane % half).astype(jnp.float32) / half)
    angles = positions[:, None] * frequency[None, :]
    sine = jnp.sin(angles)
    mixed_out = attention(
        queries,
        key_rows,
        values,
        out_gate,
        jax.nn.log_sigmoid(fwd_decay) / GATE_NORM,
        jax.nn.log_sigmoid(bwd_decay) / GATE_NORM,
        jnp.cos(angles),
        jnp.where(lane[None, :] < half, -sine, sine),
        head_gain.reshape(1, -1),
    )
    projected = jnp.dot(mixed_out, out_proj, preferred_element_type=jnp.float32)
    residual = (stream.astype(jnp.float32) + normalize(projected) * mix_gain).astype(jnp.bfloat16)
    normed = (normalize(residual.astype(jnp.float32)) * ffn_gain).astype(jnp.bfloat16)
    model_width = normed.shape[1]
    outgoing = lax.dot_general(
        pick, normed, (((0,), (0,)), ((), ())), preferred_element_type=jnp.float32
    ).astype(jnp.bfloat16)
    arrived, shared_sum = dispatch(
        outgoing.reshape(experts, capacity, model_width),
        normed,
        shared_gate,
        shared_up,
        shared_down,
    )
    return run_expert(
        arrived.reshape(experts * capacity, model_width),
        gate_parts,
        up_parts,
        down_mat,
        weights_high,
        weights_low,
        shared_sum,
        residual,
        moe_gain.reshape(1, -1),
    )


def solution(mesh):
    return jax.shard_map(
        body,
        mesh=mesh,
        in_specs=(
            P(("sp", "tp"), None),
            P("sp", "tp"),
            P("sp", "tp"),
            P("sp", "tp"),
            P("sp", "tp"),
            P("sp", "tp"),
            P("sp", "tp"),
            P("tp"),
            P(),
            P(),
            P(),
            P(),
            P(("sp", "tp"), None),
            P(("sp", "tp"), None),
            P("sp", None, "tp"),
            P("sp", None, "tp"),
            P("sp", "tp", None),
            P(None, "tp"),
            P(None, "tp"),
            P("tp", None),
        ),
        out_specs=P(("sp", "tp"), None),
        check_vma=False,
    )
```

```python
import functools

import jax
import jax.numpy as jnp
from jax import lax
from jax.experimental import pallas as pl
from jax.experimental.pallas import tpu as pltpu
from jax.sharding import PartitionSpec as P

KEY_CHANNELS = 64
DV = 128
BLK = 64
TOPK = 2


EPS = 1e-06
GATE_NORM = 16.0
ROPE_BASE = 10000.0
TOP_PRECISION = lax.Precision.HIGHEST
MESH = pl.DeviceIdType.MESH


def normalize(tensor):
    return tensor * lax.rsqrt(jnp.mean(tensor * tensor, axis=-1, keepdims=True) + EPS)


def dot_nt(left, right):
    return lax.dot_general(
        left, right, (((1,), (1,)), ((), ())), preferred_element_type=jnp.float32
    )


def dot_tn(left, right):
    return lax.dot_general(
        left, right, (((0,), (0,)), ((), ())), preferred_element_type=jnp.float32
    )


def attention_kernel(
    sp_count,
    tp_count,
    q_ref,
    k_ref,
    v_ref,
    gate_ref,
    fwd_ref,
    bwd_ref,
    cos_ref,
    sin_ref,
    gain_ref,
    out_ref,
    own_ref,
    got_ref,
    mixed_ref,
    land_ref,
    within_ref,
    key_ref,
    sums_f,
    sums_b,
    sum_send,
    sum_recv,
    row_send,
    row_recv,
):
    span, lanes = q_ref.shape
    width = v_ref.shape[1]
    heads = lanes // KEY_CHANNELS
    blocks = span // BLK
    rows_out = span // tp_count
    sp_me = lax.axis_index("sp")
    tp_me = lax.axis_index("tp")

    barrier = pltpu.get_barrier_semaphore()
    for step in range(1, sp_count):
        pl.semaphore_signal(
            barrier,
            inc=1,
            device_id=(lax.rem(sp_me + step, sp_count), tp_me),
            device_id_type=MESH,
        )
    for step in range(1, tp_count):
        pl.semaphore_signal(
            barrier,
            inc=1,
            device_id=(sp_me, lax.rem(tp_me + step, tp_count)),
            device_id_type=MESH,
        )

    row = lax.broadcasted_iota(jnp.int32, (BLK, BLK), 0)
    column = lax.broadcasted_iota(jnp.int32, (BLK, BLK), 1)
    lower = row >= column
    upper = row <= column
    lower_ones = lower.astype(jnp.float32)
    upper_ones = upper.astype(jnp.float32)
    from_lane = lax.broadcasted_iota(jnp.int32, (lanes, lanes), 0)
    to_lane = lax.broadcasted_iota(jnp.int32, (lanes, lanes), 1)
    half = KEY_CHANNELS // 2
    partner = jnp.where(lax.rem(to_lane, KEY_CHANNELS) < half, to_lane + half, to_lane - half)
    swap = (from_lane == partner).astype(jnp.bfloat16)
    own_head = (
        lax.broadcasted_iota(jnp.int32, (width, lanes), 0) // DV
        == lax.broadcasted_iota(jnp.int32, (width, lanes), 1) // KEY_CHANNELS
    )
    lane_head = lax.broadcasted_iota(jnp.int32, (BLK, lanes), 1) // KEY_CHANNELS

    def rotated(tensor, rows):
        swapped = jnp.dot(tensor, swap, preferred_element_type=jnp.float32)
        return tensor.astype(jnp.float32) * cos_ref[rows, :] + swapped * sin_ref[rows, :]

    cumul_f, cumul_b, decay_f, decay_b = [], [], [], []
    for block in range(blocks):
        rows = pl.ds(block * BLK, BLK)
        total_f = jnp.dot(
            lower_ones, fwd_ref[rows, :], precision=TOP_PRECISION, preferred_element_type=jnp.float32
        )
        total_b = jnp.dot(
            upper_ones, bwd_ref[rows, :], precision=TOP_PRECISION, preferred_element_type=jnp.float32
        )
        last_f = total_f[BLK - 1 : BLK]
        last_b = total_b[0:1]
        keys = rotated(k_ref[rows, :], rows)
        key_ref[rows, :] = keys
        value_rows = v_ref[rows, :]
        out_f = (keys * jnp.exp(last_f - total_f)).astype(jnp.bfloat16)
        out_b = (keys * jnp.exp(last_b - total_b)).astype(jnp.bfloat16)
        sums_f[block] = jnp.where(own_head, dot_tn(value_rows, out_f), 0.0)
        sums_b[block] = jnp.where(own_head, dot_tn(value_rows, out_b), 0.0)
        cumul_f.append(total_f)
        cumul_b.append(total_b)
        decay_f.append(jnp.exp(last_f))
        decay_b.append(jnp.exp(last_b))

    def packed(total):
        return sum(total[h * DV : (h + 1) * DV] for h in range(heads))

    total = sums_f[0]
    through = decay_f[0]
    for block in range(1, blocks):
        total = total * decay_f[block] + sums_f[block]
        through = through * decay_f[block]
    own_ref[0:DV, :] = packed(total).astype(jnp.bfloat16)
    own_ref[2 * DV : 2 * DV + 8, :] = jnp.broadcast_to(through, (8, lanes)).astype(jnp.bfloat16)
    total = sums_b[blocks - 1]
    through = decay_b[blocks - 1]
    for block in range(blocks - 2, -1, -1):
        total = total * decay_b[block] + sums_b[block]
        through = through * decay_b[block]
    own_ref[DV : 2 * DV, :] = packed(total).astype(jnp.bfloat16)
    own_ref[2 * DV + 8 : 2 * DV + 16, :] = jnp.broadcast_to(through, (8, lanes)).astype(
        jnp.bfloat16
    )

    pl.semaphore_wait(barrier, sp_count - 1 + tp_count - 1)
    sum_copies = []
    for step in range(1, sp_count):
        copy = pltpu.make_async_remote_copy(
            src_ref=own_ref,
            dst_ref=got_ref.at[step],
            send_sem=sum_send.at[step],
            recv_sem=sum_recv.at[step],
            device_id=(lax.rem(sp_me + step, sp_count), tp_me),
            device_id_type=MESH,
        )
        copy.start()
        sum_copies.append(copy)

    query_f, query_b = [], []
    for block in range(blocks):
        rows = pl.ds(block * BLK, BLK)
        queries = rotated(q_ref[rows, :], rows) * KEY_CHANNELS ** (-0.5)
        keys = key_ref[rows, :]
        total_f, total_b = cumul_f[block], cumul_b[block]
        middle_f = total_f[BLK // 2 - 1 : BLK // 2]
        middle_b = total_b[BLK // 2 : BLK // 2 + 1]
        scaled_qf = queries * jnp.exp(total_f - middle_f)
        scaled_qb = queries * jnp.exp(total_b - middle_b)
        scaled_kf = (keys * jnp.exp(middle_f - total_f)).astype(jnp.bfloat16)
        scaled_kb = (keys * jnp.exp(middle_b - total_b)).astype(jnp.bfloat16)
        query_f.append((queries * jnp.exp(total_f)).astype(jnp.bfloat16))
        query_b.append((queries * jnp.exp(total_b)).astype(jnp.bfloat16))
        for h in range(heads):
            mine = lane_head == h
            scores_f = dot_nt(jnp.where(mine, scaled_qf, 0.0).astype(jnp.bfloat16), scaled_kf)
            scores_b = dot_nt(jnp.where(mine, scaled_qb, 0.0).astype(jnp.bfloat16), scaled_kb)
            scores = jnp.where(lower, scores_f, 0.0) + jnp.where(upper, scores_b, 0.0)
            within_ref[rows, h * DV : (h + 1) * DV] = jnp.dot(
                scores.astype(jnp.bfloat16),
                v_ref[rows, h * DV : (h + 1) * DV],
                preferred_element_type=jnp.float32,
            )

    for copy in sum_copies:
        copy.wait()
    carry_f = jnp.zeros((DV, lanes), jnp.float32)
    carry_b = jnp.zeros((DV, lanes), jnp.float32)
    for step in range(sp_count - 1, 0, -1):
        state = got_ref[step, 0:DV, :].astype(jnp.float32)
        through = got_ref[step, 2 * DV : 2 * DV + 16, :].astype(jnp.float32)[0:1]
        carry_f = jnp.where(step <= sp_me, carry_f * through + state, carry_f)
    for step in range(1, sp_count):
        state = got_ref[step, DV : 2 * DV, :].astype(jnp.float32)
        through = got_ref[step, 2 * DV : 2 * DV + 16, :].astype(jnp.float32)[8:9]
        carry_b = jnp.where(step > sp_me, carry_b * through + state, carry_b)

    def unpacked(carry):
        return jnp.where(own_head, jnp.concatenate([carry] * heads, axis=0), 0.0)

    state = unpacked(carry_f)
    for block in range(blocks):
        rows = pl.ds(block * BLK, BLK)
        within_ref[rows, :] += dot_nt(query_f[block], state.astype(jnp.bfloat16))
        if block < blocks - 1:
            state = state * decay_f[block] + sums_f[block]
    state = unpacked(carry_b)
    for block in range(blocks - 1, -1, -1):
        rows = pl.ds(block * BLK, BLK)
        attended = within_ref[rows, :] + dot_nt(query_b[block], state.astype(jnp.bfloat16))
        if block > 0:
            state = state * decay_b[block] + sums_b[block]
        for h in range(heads):
            part = attended[:, h * DV : (h + 1) * DV]
            square = jnp.mean(part * part, axis=-1, keepdims=True)
            gate = gate_ref[rows, h * DV : (h + 1) * DV].astype(jnp.float32)
            mixed_ref[rows, h * DV : (h + 1) * DV] = (
                part
                * lax.rsqrt(square + EPS)
                * gain_ref[:, h * DV : (h + 1) * DV]
                * (gate / (1.0 + jnp.exp(-gate)))
            ).astype(jnp.bfloat16)

    row_copies = []
    for step in range(1, tp_count):
        target = lax.rem(tp_me + step, tp_count)
        copy = pltpu.make_async_remote_copy(
            src_ref=mixed_ref.at[pl.ds(pl.multiple_of(target * rows_out, rows_out), rows_out)],
            dst_ref=land_ref.at[tp_me],
            send_sem=row_send.at[step],
            recv_sem=row_recv.at[step],
            device_id=(sp_me, target),
            device_id_type=MESH,
        )
        copy.start()
        row_copies.append(copy)
    land_ref[tp_me] = mixed_ref[pl.ds(pl.multiple_of(tp_me * rows_out, rows_out), rows_out), :]
    for copy in row_copies:
        copy.wait()
    for source in range(tp_count):
        out_ref[:, source * width : (source + 1) * width] = land_ref[source]


def attention(queries, key_rows, values, out_gate, fwd_log, bwd_log, cosine, signed_sine, gain):
    sp_count = lax.axis_size("sp")
    tp_count = lax.axis_size("tp")
    span, lanes = queries.shape
    width = values.shape[1]
    rows_out = span // tp_count
    blocks = span // BLK
    vmem = pl.BlockSpec(memory_space=pltpu.VMEM)
    return pl.pallas_call(
        functools.partial(attention_kernel, sp_count, tp_count),
        out_shape=jax.ShapeDtypeStruct((rows_out, tp_count * width), jnp.bfloat16),
        in_specs=[vmem] * 9,
        out_specs=vmem,
        scratch_shapes=[
            pltpu.VMEM((2 * DV + 16, lanes), jnp.bfloat16),
            pltpu.VMEM((sp_count, 2 * DV + 16, lanes), jnp.bfloat16),
            pltpu.VMEM((span, width), jnp.bfloat16),
            pltpu.VMEM((tp_count, rows_out, width), jnp.bfloat16),
            pltpu.VMEM((span, width), jnp.float32),
            pltpu.VMEM((span, lanes), jnp.float32),
            pltpu.VMEM((blocks, width, lanes), jnp.float32),
            pltpu.VMEM((blocks, width, lanes), jnp.float32),
            pltpu.SemaphoreType.DMA((sp_count,)),
            pltpu.SemaphoreType.DMA((sp_count,)),
            pltpu.SemaphoreType.DMA((tp_count,)),
            pltpu.SemaphoreType.DMA((tp_count,)),
        ],
        compiler_params=pltpu.CompilerParams(collective_id=0, has_side_effects=True),
    )(queries, key_rows, values, out_gate, fwd_log, bwd_log, cosine, signed_sine, gain)


def dispatch_kernel(
    sp_count,
    tp_count,
    outgoing_ref,
    rows_ref,
    gate_ref,
    up_ref,
    down_ref,
    arrived_ref,
    shared_ref,
    part_ref,
    block_land,
    row_land,
    block_send,
    block_recv,
    row_send,
    row_recv,
):
    sp_me = lax.axis_index("sp")
    tp_me = lax.axis_index("tp")

    def sp_peer(step):
        return (lax.rem(sp_me + step, sp_count), tp_me)

    def tp_peer(step):
        return (sp_me, lax.rem(tp_me + step, tp_count))

    barrier = pltpu.get_barrier_semaphore()
    for step in range(1, sp_count):
        pl.semaphore_signal(barrier, inc=1, device_id=sp_peer(step), device_id_type=MESH)
    for step in range(1, tp_count):
        pl.semaphore_signal(barrier, inc=1, device_id=tp_peer(step), device_id_type=MESH)
    pl.semaphore_wait(barrier, sp_count - 1 + tp_count - 1)

    row_copies, block_copies = [], []
    for step in range(1, tp_count):
        copy = pltpu.make_async_remote_copy(
            src_ref=rows_ref,
            dst_ref=row_land.at[step],
            send_sem=row_send.at[step],
            recv_sem=row_recv.at[step],
            device_id=tp_peer(step),
            device_id_type=MESH,
        )
        copy.start()
        row_copies.append(copy)
    for step in range(1, sp_count):
        copy = pltpu.make_async_remote_copy(
            src_ref=outgoing_ref.at[lax.rem(sp_me + step, sp_count)],
            dst_ref=block_land.at[sp_me],
            send_sem=block_send.at[step],
            recv_sem=block_recv.at[step],
            device_id=sp_peer(step),
            device_id_type=MESH,
        )
        copy.start()
        block_copies.append(copy)
    block_land[sp_me] = outgoing_ref[sp_me]

    def partial(rows):
        hidden = jax.nn.silu(
            jnp.dot(rows, gate_ref[...], preferred_element_type=jnp.float32)
        ) * jnp.dot(rows, up_ref[...], preferred_element_type=jnp.float32)
        return jnp.dot(
            hidden.astype(jnp.bfloat16), down_ref[...], preferred_element_type=jnp.float32
        )

    shared_ref[...] = partial(rows_ref[...])
    for step in range(1, tp_count):
        row_copies[step - 1].wait()
        part_ref[step] = partial(row_land[step]).astype(jnp.bfloat16)
    part_ref[0] = jnp.zeros(part_ref.shape[1:], part_ref.dtype)
    for copy in block_copies:
        copy.wait()
    arrived_ref[...] = block_land[...]


def dispatch(outgoing, normed, shared_gate, shared_up, shared_down):
    sp_count = lax.axis_size("sp")
    tp_count = lax.axis_size("tp")
    vmem = pl.BlockSpec(memory_space=pltpu.VMEM)
    several = pltpu.VMEM((tp_count,) + normed.shape, normed.dtype)
    return pl.pallas_call(
        functools.partial(dispatch_kernel, sp_count, tp_count),
        out_shape=(
            jax.ShapeDtypeStruct(outgoing.shape, outgoing.dtype),
            jax.ShapeDtypeStruct(normed.shape, jnp.float32),
            jax.ShapeDtypeStruct((tp_count,) + normed.shape, normed.dtype),
        ),
        in_specs=[vmem] * 5,
        out_specs=(vmem, vmem, vmem),
        scratch_shapes=[
            pltpu.VMEM(outgoing.shape, outgoing.dtype),
            several,
            pltpu.SemaphoreType.DMA((sp_count,)),
            pltpu.SemaphoreType.DMA((sp_count,)),
            pltpu.SemaphoreType.DMA((tp_count,)),
            pltpu.SemaphoreType.DMA((tp_count,)),
        ],
        compiler_params=pltpu.CompilerParams(collective_id=1, has_side_effects=True),
    )(outgoing, normed, shared_gate, shared_up, shared_down)


def expert_kernel(
    sp_count,
    tp_count,
    rows_ref,
    gate_hbm,
    up_hbm,
    down_hbm,
    high_ref,
    low_ref,
    shared_ref,
    part_ref,
    residual_ref,
    gain_ref,
    out_ref,
    gate_ref,
    up_ref,
    down_ref,
    total_ref,
    done_ref,
    back_ref,
    part_land,
    weight_sem,
    send_sem,
    recv_sem,
    part_send,
    part_recv,
):
    sp_me = lax.axis_index("sp")
    tp_me = lax.axis_index("tp")
    groups, _, width = gate_ref.shape
    capacity = done_ref.shape[1]

    fetches = []
    for group in range(groups):
        cut = pl.ds(group * width, width)
        trio = (
            pltpu.make_async_copy(gate_hbm.at[group], gate_ref.at[group], weight_sem.at[0, group]),
            pltpu.make_async_copy(up_hbm.at[group], up_ref.at[group], weight_sem.at[1, group]),
            pltpu.make_async_copy(down_hbm.at[cut], down_ref.at[cut], weight_sem.at[2, group]),
        )
        for copy in trio:
            copy.start()
        fetches.append(trio)

    barrier = pltpu.get_barrier_semaphore()
    for step in range(1, sp_count):
        pl.semaphore_signal(
            barrier,
            inc=1,
            device_id=(lax.rem(sp_me + step, sp_count), tp_me),
            device_id_type=MESH,
        )

    for step in range(1, tp_count):
        pl.semaphore_signal(
            barrier,
            inc=1,
            device_id=(sp_me, lax.rem(tp_me + step, tp_count)),
            device_id_type=MESH,
        )
    pl.semaphore_wait(barrier, sp_count - 1 + tp_count - 1)
    part_copies = []
    for step in range(1, tp_count):
        copy = pltpu.make_async_remote_copy(
            src_ref=part_ref.at[step],
            dst_ref=part_land.at[step],
            send_sem=part_send.at[step],
            recv_sem=part_recv.at[step],
            device_id=(sp_me, lax.rem(tp_me + tp_count - step, tp_count)),
            device_id_type=MESH,
        )
        copy.start()
        part_copies.append(copy)

    for group in range(groups):
        for copy in fetches[group]:
            copy.wait()
        hidden = (
            jax.nn.silu(jnp.dot(rows_ref[...], gate_ref[group], preferred_element_type=jnp.float32))
            * jnp.dot(rows_ref[...], up_ref[group], preferred_element_type=jnp.float32)
        ).astype(jnp.bfloat16)
        piece = jnp.dot(
            hidden,
            down_ref[group * width : (group + 1) * width, :],
            preferred_element_type=jnp.float32,
        )
        if group == 0:
            total_ref[...] = piece
        else:
            total_ref[...] += piece
    for source in range(sp_count):
        done_ref[source] = total_ref[source * capacity : (source + 1) * capacity, :].astype(
            done_ref.dtype
        )

    copies = []
    for step in range(1, sp_count):
        target = lax.rem(sp_me + step, sp_count)
        copy = pltpu.make_async_remote_copy(
            src_ref=done_ref.at[target],
            dst_ref=back_ref.at[sp_me],
            send_sem=send_sem.at[step],
            recv_sem=recv_sem.at[step],
            device_id=(target, tp_me),
            device_id_type=MESH,
        )
        copy.start()
        copies.append(copy)
    back_ref[sp_me] = done_ref[sp_me]
    for copy in copies:
        copy.wait()

    mixture = shared_ref[...]
    for step in range(1, tp_count):
        part_copies[step - 1].wait()
        mixture = mixture + part_land[step].astype(jnp.float32)
    for expert in range(sp_count):
        mixture = mixture + jnp.dot(
            high_ref[expert], back_ref[expert], preferred_element_type=jnp.float32
        )
        mixture = mixture + jnp.dot(
            low_ref[expert], back_ref[expert], preferred_element_type=jnp.float32
        )
    square = jnp.mean(mixture * mixture, axis=-1, keepdims=True)
    out_ref[...] = (
        residual_ref[...].astype(jnp.float32)
        + mixture * lax.rsqrt(square + EPS) * gain_ref[...]
    ).astype(out_ref.dtype)


def run_expert(rows, gate_parts, up_parts, down_mat, high, low, shared_sum, parts, residual, gain):
    sp_count = lax.axis_size("sp")
    groups = gate_parts.shape[0]
    vmem = pl.BlockSpec(memory_space=pltpu.VMEM)
    hbm = pl.BlockSpec(memory_space=pl.ANY)
    blocked = pltpu.VMEM((sp_count, rows.shape[0] // sp_count, rows.shape[1]), rows.dtype)
    return pl.pallas_call(
        functools.partial(expert_kernel, sp_count, lax.axis_size("tp")),
        out_shape=jax.ShapeDtypeStruct(residual.shape, residual.dtype),
        in_specs=[vmem, hbm, hbm, hbm] + [vmem] * 6,
        out_specs=vmem,
        scratch_shapes=[
            pltpu.VMEM(gate_parts.shape, gate_parts.dtype),
            pltpu.VMEM(up_parts.shape, up_parts.dtype),
            pltpu.VMEM(down_mat.shape, down_mat.dtype),
            pltpu.VMEM(rows.shape, jnp.float32),
            blocked,
            blocked,
            pltpu.VMEM(parts.shape, parts.dtype),
            pltpu.SemaphoreType.DMA((3, groups)),
            pltpu.SemaphoreType.DMA((sp_count,)),
            pltpu.SemaphoreType.DMA((sp_count,)),
            pltpu.SemaphoreType.DMA((parts.shape[0],)),
            pltpu.SemaphoreType.DMA((parts.shape[0],)),
        ],
        compiler_params=pltpu.CompilerParams(collective_id=2, has_side_effects=True),
    )(rows, gate_parts, up_parts, down_mat, high, low, shared_sum, parts, residual, gain)


def slot_map(route_block, experts, capacity):
    tokens, choices = route_block.shape
    flat_ids = route_block.reshape(-1)
    total = flat_ids.shape[0]
    onehot = (flat_ids[:, None] == jnp.arange(experts, dtype=jnp.int32)[None, :]).astype(
        jnp.bfloat16
    )
    earlier = (jnp.arange(total)[:, None] > jnp.arange(total)[None, :]).astype(jnp.bfloat16)
    before = jnp.dot(earlier, onehot, preferred_element_type=jnp.float32)
    slot_ids = jnp.sum(before * onehot.astype(jnp.float32), axis=1).astype(jnp.int32)
    return (flat_ids * capacity + slot_ids).reshape(tokens, choices)


def body(
    stream,
    queries,
    key_rows,
    values,
    out_gate,
    fwd_decay,
    bwd_decay,
    head_gain,
    out_proj,
    mix_gain,
    ffn_gain,
    moe_gain,
    routes,
    route_weight,
    expert_gate,
    expert_up,
    expert_down,
    shared_gate,
    shared_up,
    shared_down,
):
    tokens_here = stream.shape[0]
    span_rows = queries.shape[0]
    experts = lax.axis_size("sp")
    capacity = max(2, 3 * tokens_here * TOPK // (2 * experts))
    gate_parts = lax.all_gather(expert_gate[0], "tp")
    up_parts = lax.all_gather(expert_up[0], "tp")
    down_mat = lax.all_gather(expert_down[0], "tp", axis=0, tiled=True)
    rows_of = slot_map(routes, experts, capacity)
    slots = jnp.arange(experts * capacity, dtype=jnp.int32)
    taken = rows_of[:, :, None] == slots[None, None, :]
    pick = jnp.any(taken, axis=1).astype(jnp.bfloat16)
    weights = jnp.sum(jnp.where(taken, route_weight[:, :, None], 0.0), axis=1)
    weights = weights.reshape(tokens_here, experts, capacity).transpose(1, 0, 2)
    weights_high = weights.astype(jnp.bfloat16)
    weights_low = (weights - weights_high.astype(jnp.float32)).astype(jnp.bfloat16)
    offset = lax.axis_index("sp") * span_rows
    positions = (offset + jnp.arange(span_rows, dtype=jnp.int32)).astype(jnp.float32)
    lanes = queries.shape[1]
    half = KEY_CHANNELS // 2
    lane = jnp.arange(lanes, dtype=jnp.int32) % KEY_CHANNELS
    frequency = ROPE_BASE ** (-(lane % half).astype(jnp.float32) / half)
    angles = positions[:, None] * frequency[None, :]
    sine = jnp.sin(angles)
    mixed_out = attention(
        queries,
        key_rows,
        values,
        out_gate,
        jax.nn.log_sigmoid(fwd_decay) / GATE_NORM,
        jax.nn.log_sigmoid(bwd_decay) / GATE_NORM,
        jnp.cos(angles),
        jnp.where(lane[None, :] < half, -sine, sine),
        head_gain.reshape(1, -1),
    )
    projected = jnp.dot(mixed_out, out_proj, preferred_element_type=jnp.float32)
    residual = (stream.astype(jnp.float32) + normalize(projected) * mix_gain).astype(jnp.bfloat16)
    normed = (normalize(residual.astype(jnp.float32)) * ffn_gain).astype(jnp.bfloat16)
    model_width = normed.shape[1]
    outgoing = lax.dot_general(
        pick, normed, (((0,), (0,)), ((), ())), preferred_element_type=jnp.float32
    ).astype(jnp.bfloat16)
    arrived, shared_sum, parts = dispatch(
        outgoing.reshape(experts, capacity, model_width),
        normed,
        shared_gate,
        shared_up,
        shared_down,
    )
    return run_expert(
        arrived.reshape(experts * capacity, model_width),
        gate_parts,
        up_parts,
        down_mat,
        weights_high,
        weights_low,
        shared_sum,
        parts,
        residual,
        moe_gain.reshape(1, -1),
    )


def solution(mesh):
    return jax.shard_map(
        body,
        mesh=mesh,
        in_specs=(
            P(("sp", "tp"), None),
            P("sp", "tp"),
            P("sp", "tp"),
            P("sp", "tp"),
            P("sp", "tp"),
            P("sp", "tp"),
            P("sp", "tp"),
            P("tp"),
            P(),
            P(),
            P(),
            P(),
            P(("sp", "tp"), None),
            P(("sp", "tp"), None),
            P("sp", None, "tp"),
            P("sp", None, "tp"),
            P("sp", "tp", None),
            P(None, "tp"),
            P(None, "tp"),
            P("tp", None),
        ),
        out_specs=P(("sp", "tp"), None),
        check_vma=False,
    )
```
